512 devices in a mesh: sp: 16 (over z), dp: 32 (over y, x, core).
Axes of the slice: x: 4, y: 4, z: 16, core: 2. Of those that a mesh axis runs over, the one named last changes fastest.
Arguments:
- inputs: bfloat16 [32, 2048, 2048], P('dp', 'sp'), may hold values from -6 to 6
- queries: bfloat16 [32, 2048, 1024], P('dp', 'sp'), may hold values from -6 to 6
- keys: bfloat16 [32, 2048, 1024], P('dp', 'sp'), may hold values from -1.5 to 1.5
- values: bfloat16 [32, 2048, 1024], P('dp', 'sp'), may hold values from -6 to 6
- log_decay: bfloat16 [32, 2048, 1024], P('dp', 'sp'), may hold values from -0.1 to 0, as said below
- cotangent: bfloat16 [32, 2048, 1024], P('dp', 'sp'), may hold values from -0.59765625 to 0.59765625
- value_weight: bfloat16 [2048, 1024], P('dp'), may hold values from -0.125 to 0.125
Outputs:
- grad_queries: bfloat16 [32, 2048, 1024], P('dp', 'sp')
- grad_keys: bfloat16 [32, 2048, 1024], P('dp', 'sp')
- grad_decay: bfloat16 [32, 2048, 1024], P('dp', 'sp')
- grad_inputs: bfloat16 [32, 2048, 2048], P('dp', 'sp')
- grad_weight: float32 [2048, 1024], P('dp')
The draws below stay inside these ranges and needn't reach their ends.
Inputs may be any that keep to these rules, and one draw needn't show every extreme that they name: `log_decay`: the log decays are negative; per key channel and sequence they differ between positions.
All inputs are finite; a program needn't handle non-finite values.
Results may differ from the reference program's by a relative error of at most 0.015.
Values may be sent and summed in bfloat16 or wider, within the bound.
A program may use at most 128 MiB of HBM per device.

```python
import math
import jax
import jax.numpy as jnp
from jax import lax

D = 2048
HEADS = 16
HEAD_DIM = 64
BLOCK = 128
HALF = 32
GROUPS = 32
WIDTH = 1024
SEQ = 2048
SEQS = 32


def draw_log_decay(key, part):
    keys_list = jax.random.split(key, 5)
    share = 0.5
    slow_pick = jax.random.uniform(keys_list[0], (SEQS, 1, WIDTH), jnp.float32) < share
    fast_rate = jax.random.uniform(keys_list[1], (SEQS, 1, WIDTH), jnp.float32, 1.0 / 50.0, 1.0 / 30.0)
    slow_rate = jax.random.uniform(keys_list[2], (SEQS, 1, WIDTH), jnp.float32, 0.2, 0.5) / SEQ
    base_rate = jnp.where(slow_pick, slow_rate, fast_rate)
    block_count = SEQ // BLOCK
    block_factor = jnp.exp(jax.random.uniform(keys_list[3], (SEQS, block_count, 1, WIDTH), jnp.float32, -math.log(2.0), math.log(2.0)))
    block_factor = jnp.broadcast_to(block_factor, (SEQS, block_count, BLOCK, WIDTH)).reshape(SEQS, SEQ, WIDTH)
    token_factor = jnp.exp(jax.random.uniform(keys_list[4], (SEQS, SEQ, WIDTH), jnp.float32, math.log(0.7), math.log(1.4)))
    return (-(base_rate * block_factor * token_factor)).astype(jnp.bfloat16)


def levels(stream_key, extent, cuts, low, high):
    gain = 1.0
    for axis_at, parts in cuts:
        steps = jax.random.uniform(jax.random.fold_in(jax.random.fold_in(stream_key, 6), axis_at), (parts,), jnp.float32, low / len(cuts), high / len(cuts))
        gain = gain * jnp.repeat(jnp.exp(steps), extent[axis_at] // parts).reshape((-1,) + (1,) * (len(extent) - 1 - axis_at))
    return gain


def scatter_about(rng, shape, scale, limit, cuts=(), dtype=jnp.bfloat16):
    result = jax.random.normal(rng, shape, jnp.float32) * scale
    if len(cuts) > 0:
        result = levels(rng, shape, cuts, -0.22, 0.18) * result
    return jnp.clip(result, min=-limit, max=limit).astype(dtype)


def setup_inputs(seed: int = 0) -> dict:
    key_of = jax.random.split(jax.random.key(seed), 8)
    inputs = scatter_about(key_of[0], (SEQS, SEQ, D), 1.0, 6.0, ((0, 32), (1, 16)))
    queries = scatter_about(key_of[1], (SEQS, SEQ, WIDTH), 1.0, 6.0, ((0, 32), (1, 16)))
    keys = scatter_about(key_of[2], (SEQS, SEQ, WIDTH), 0.25, 1.5, ((0, 32), (1, 16)))
    values = scatter_about(key_of[3], (SEQS, SEQ, WIDTH), 1.0, 6.0, ((0, 32), (1, 16)))
    log_decay = draw_log_decay(jax.random.fold_in(key_of[7], 71), 0)
    cotangent = scatter_about(key_of[5], (SEQS, SEQ, WIDTH), 0.1, 0.59765625, ((0, 32), (1, 16)))
    value_weight = scatter_about(key_of[6], (D, WIDTH), D ** -0.5, 0.125, ((0, 32),))
    return {"inputs": inputs, "queries": queries, "keys": keys, "values": values, "log_decay": log_decay, "cotangent": cotangent, "value_weight": value_weight}


def combine(earlier, later):
    first_decay, first_state = earlier
    second_decay, second_state = later
    return (first_decay * second_decay, second_decay[..., None] * first_state + second_state)

def carry_scan(decays, updates):
    return lax.associative_scan(combine, (decays, updates), axis=0)[1]

def to_blocks(rows, num_blocks):
    length, groups, width = rows.shape
    return jnp.transpose(rows.astype(jnp.float32).reshape(num_blocks, BLOCK, groups, width), (0, 2, 3, 1))

def mixing(query_rows, key_rows, value_rows, gate_rows):
    length, groups, key_width = query_rows.shape
    value_width = value_rows.shape[2]
    num_blocks = length // BLOCK
    scaled_query = to_blocks(query_rows, num_blocks) * HEAD_DIM ** (-0.5)
    key_float = to_blocks(key_rows, num_blocks)
    value_float = to_blocks(value_rows, num_blocks)
    gate_float = to_blocks(gate_rows, num_blocks)
    running = jnp.cumsum(gate_float, axis=3)
    exclusive = running - gate_float
    block_end = running[..., -1]
    lower_mask = jnp.tril(jnp.ones((BLOCK, BLOCK), jnp.float32))
    upper_mask = lower_mask.T
    query_fwd = scaled_query * jnp.exp(running)
    key_fwd = key_float * jnp.exp(-running)
    scores_fwd = jnp.einsum('ngcr,ngcs->ngrs', query_fwd, key_fwd) * lower_mask
    key_end = key_float * jnp.exp(block_end[..., None] - running)
    states = carry_scan(jnp.exp(block_end), jnp.einsum('ngcs,ngvs->ngcv', key_end, value_float))
    before = jnp.concatenate([jnp.zeros_like(states[:1]), states[:-1]], axis=0)
    out_fwd = jnp.einsum('ngrs,ngvs->ngvr', scores_fwd, value_float) + jnp.einsum('ngcr,ngcv->ngvr', query_fwd, before)
    query_bwd = scaled_query * jnp.exp(-exclusive)
    key_bwd = key_float * jnp.exp(exclusive)
    scores_bwd = jnp.einsum('ngcr,ngcs->ngrs', query_bwd, key_bwd) * upper_mask
    rights = jnp.flip(carry_scan(jnp.flip(jnp.exp(block_end), 0), jnp.flip(jnp.einsum('ngcs,ngvs->ngcv', key_bwd, value_float), 0)), 0)
    after = jnp.concatenate([rights[1:], jnp.zeros_like(rights[:1])], axis=0)
    query_read = scaled_query * jnp.exp(block_end[..., None] - exclusive)
    out_bwd = jnp.einsum('ngrs,ngvs->ngvr', scores_bwd, value_float) + jnp.einsum('ngcr,ngcv->ngvr', query_read, after)
    total = out_fwd + out_bwd
    return jnp.transpose(total, (0, 3, 1, 2)).reshape(length, groups, value_width)

def reference(inputs, queries, keys, values, log_decay, cotangent, value_weight):
    seq_len = queries.shape[1]
    width = queries.shape[2]

    def per_group(array):
        spread = jnp.broadcast_to(array.reshape(seq_len, HEADS, 1, HEAD_DIM), (seq_len, HEADS, 2, HEAD_DIM))
        return spread.reshape(seq_len, GROUPS, HEAD_DIM)

    def one_sequence(pieces):
        query_seq, key_seq, value_seq, gate_seq, upstream = pieces
        _, pullback = jax.vjp(mixing, query_seq.reshape(seq_len, GROUPS, HALF), key_seq.reshape(seq_len, GROUPS, HALF), per_group(value_seq), gate_seq.reshape(seq_len, GROUPS, HALF))
        grad_q, grad_k, grad_v, grad_g = pullback(per_group(upstream).astype(jnp.float32))
        value_sum = lax.optimization_barrier(jnp.sum(grad_v.astype(jnp.bfloat16).astype(jnp.float32).reshape(seq_len, HEADS, 2, HEAD_DIM), axis=2))
        return (grad_q.astype(jnp.bfloat16).reshape(seq_len, width), grad_k.astype(jnp.bfloat16).reshape(seq_len, width), grad_g.astype(jnp.bfloat16).reshape(seq_len, width), value_sum.astype(jnp.bfloat16).reshape(seq_len, width))
    grad_queries, grad_keys, grad_decay, value_grad = lax.map(one_sequence, (queries, keys, values, log_decay, cotangent))
    flat_inputs = inputs.reshape(-1, inputs.shape[2])
    flat_grad = value_grad.reshape(-1, width)
    grad_inputs = jnp.dot(flat_grad, value_weight.T, preferred_element_type=jnp.float32).astype(jnp.bfloat16).reshape(inputs.shape)
    grad_weight = jnp.dot(flat_inputs.T, flat_grad, preferred_element_type=jnp.float32)
    return (grad_queries, grad_keys, grad_decay, grad_inputs, grad_weight)
```

```python
import functools

import jax
import jax.numpy as jnp
from jax import lax
from jax.experimental import pallas as pl
from jax.experimental.pallas import tpu as pltpu
from jax.sharding import PartitionSpec as P

MESH = pl.DeviceIdType.MESH
F32 = jnp.float32
BF16 = jnp.bfloat16
BLOCK = 128
WIDTH = 1024
HALF = WIDTH // 2
PAIRS = WIDTH // 128
CHUNKS = 2 * PAIRS
HEAD_DIM = 64


def nn(a, b):
    return lax.dot_general(a, b, (((1,), (0,)), ((), ())), preferred_element_type=F32)


def nt(a, b):
    return lax.dot_general(a, b, (((1,), (1,)), ((), ())), preferred_element_type=F32)


def tn(a, b):
    return lax.dot_general(a, b, (((0,), (0,)), ((), ())), preferred_element_type=F32)


def lanes(start, size):
    return pl.ds(pl.multiple_of(start, 128), size)


def kernel(
    nz, nq,
    q_ref, k_ref, v_ref, g_ref, cot_ref, x_ref, w_ref,
    dq_ref, dk_ref, dg_ref, gi_ref, gw_ref,
    run_s, end_s, qf_s, kf_s, qb_s, kb_s, loc_s, raw_s, send_s, recv_s,
    dqf_s, dqb_s, dkf_s, dkb_s, dv_s, dvb_s,
    wv_s, xg_s, dvg_s, part_s, pb_s, s2_s, acc_s, zb_s, zr_s, rb_s, gr_s,
    chain_ss, chain_rs, w0_ss, w0_rs, w_loc, w1_ss, w1_rs, w2_ss, w2_rs, w3_ss, w3_rs,
    x_ss, x_rs, dv_ss, dv_rs, s2_ss, s2_rs, zr_ss, zr_rs, za_ss, za_rs,
):
    z = lax.axis_index("sp")
    d = lax.axis_index("dp")
    c = lax.rem(d, 2)
    chip = lax.div(d, 2)
    xx = lax.rem(chip, nq)
    yy = lax.div(chip, nq)
    pa = xx * (1 - c) + yy * c
    pb = yy * (1 - c) + xx * c

    def chip_at(a, b):
        return (b * nq + a) * (1 - c) + (a * nq + b) * c

    def there(chip_id, core, at_z=None):
        return {"sp": z if at_z is None else at_z, "dp": chip_id * 2 + core}

    def turned(at, i, n):
        return lax.rem(at + i, n)

    barrier = pltpu.get_barrier_semaphore()
    greeted = 0
    for i in range(1, nq):
        for core in range(2):
            for other in (yy * nq + turned(xx, i, nq), turned(yy, i, nq) * nq + xx):
                pl.semaphore_signal(barrier, inc=1, device_id=there(other, core), device_id_type=MESH)
                greeted += 1
    pl.semaphore_signal(barrier, inc=1, device_id=there(chip, 1 - c), device_id_type=MESH)
    for step in (1, nz - 1):
        pl.semaphore_signal(
            barrier, inc=1, device_id=there(chip, c, turned(z, step, nz)), device_id_type=MESH
        )
    pl.semaphore_wait(barrier, greeted + 3)

    def remote(src, dst, ss, rs, device):
        return pltpu.make_async_remote_copy(
            src_ref=src, dst_ref=dst, send_sem=ss, recv_sem=rs, device_id=device, device_id_type=MESH
        )

    w_here = pltpu.make_async_copy(
        w_ref.at[:, lanes(c * HALF, HALF)],
        wv_s.at[c, chip, pl.ds(pl.multiple_of(c * 64, 64), 64), :],
        w_loc,
    )
    w_here.start()
    w0 = remote(
        w_ref.at[:, lanes((1 - c) * HALF, HALF)],
        wv_s.at[1 - c, chip, pl.ds(pl.multiple_of(c * 64, 64), 64), :],
        w0_ss, w0_rs, there(chip, 1 - c),
    )
    w0.start()

    x_slot = (xx * 2 + c, yy * 2 + c)

    def x_copies(role, i):
        if role == 0:
            to = turned(xx, i, nq)
            target = there(yy * nq + to, 0)
            pieces = [
                (
                    x_ref.at[:, lanes((b * nq + to) * 128, 128)],
                    xg_s.at[x_slot[0], :, pl.ds(b * 128, 128)],
                )
                for b in range(nq)
            ]
        else:
            to = turned(yy, i, nq)
            target = there(to * nq + xx, 1)
            pieces = [(x_ref.at[:, lanes(to * nq * 128, nq * 128)], xg_s.at[x_slot[1]])]
        return target, pieces

    def send_x(role, i):
        target, pieces = x_copies(role, i)

        def away():
            for src, dst in pieces:
                remote(src, dst, x_ss.at[role, i], x_rs.at[x_slot[role]], target).start()

        def at_home():
            for src, dst in pieces:
                pltpu.make_async_copy(src, dst, x_rs.at[x_slot[role]]).start()

        if i == 0:
            pl.when(c != role)(away)
            pl.when(c == role)(at_home)
        else:
            away()

    for role in range(2):
        for i in range(nq):
            send_x(role, i)

    row = lax.broadcasted_iota(jnp.int32, (BLOCK, BLOCK), 0)
    col = lax.broadcasted_iota(jnp.int32, (BLOCK, BLOCK), 1)
    left_half = lax.broadcasted_iota(jnp.int32, (64, 128), 1) < 64
    lane = lax.broadcasted_iota(jnp.int32, (BLOCK, 128), 1)
    mask0 = jnp.where(lane < 64, 1.0, 0.0).astype(BF16)
    mask1 = jnp.where(lane < 64, 0.0, 1.0).astype(BF16)
    upto = jnp.where(row >= col, 1.0, 0.0).astype(BF16)
    onward = jnp.where(row <= col, 1.0, 0.0).astype(BF16)

    def diagonal(m):
        return jnp.where(left_half, m[:64], m[64:])

    def local_states(p, _):
        at = lanes(p * 128, 128)
        gate = g_ref[:, at]
        running = nn(upto, gate)
        exclusive = running - gate.astype(F32)
        run_s[:, at] = running
        end = jnp.exp(running[BLOCK - 1 : BLOCK])
        end_s[:, at] = jnp.broadcast_to(end, (8, 128))
        query = q_ref[:, at].astype(F32) * HEAD_DIM ** (-0.5)
        key = k_ref[:, at].astype(F32)
        qf = (query * jnp.exp(running)).astype(BF16)
        kf = (key * jnp.exp(-running)).astype(BF16)
        qb = (query * jnp.exp(-exclusive)).astype(BF16)
        kb = (key * jnp.exp(exclusive)).astype(BF16)
        qf_s[:, at] = qf
        kf_s[:, at] = kf
        qb_s[:, at] = qb
        kb_s[:, at] = kb
        value = v_ref[:, at]
        cot = cot_ref[:, at]
        uh = diagonal(tn(value, kf))
        wb = diagonal(tn(cot, qb))
        raw_s[2 * p] = uh
        raw_s[2 * p + 1] = wb
        loc_s[0, 2 * p] = uh * end
        loc_s[0, 2 * p + 1] = wb * end
        loc_s[1, 2 * p] = diagonal(tn(cot, qf))
        loc_s[1, 2 * p + 1] = diagonal(tn(value, kb))
        return 0

    lax.fori_loop(0, PAIRS, local_states, 0)

    w_here.wait()
    w0.wait()
    w1 = [
        remote(
            wv_s.at[c, chip], wv_s.at[c, chip], w1_ss.at[i - 1], w1_rs.at[i - 1],
            there(chip_at(turned(pa, i, nq), pb), c),
        )
        for i in range(1, nq)
    ]
    for copy in w1:
        copy.start()

    def both(a):
        return jnp.concatenate([a * mask0, a * mask1], axis=0)

    row2 = lax.broadcasted_iota(jnp.int32, (BLOCK, 256), 0)
    col2 = lax.rem(lax.broadcasted_iota(jnp.int32, (BLOCK, 256), 1), 128)
    lower = row2 >= col2
    upper = row2 <= col2

    def own_part(p, _):
        at = lanes(p * 128, 128)
        value = v_ref[:, at]
        cot = cot_ref[:, at]
        qf, kf, qb, kb = qf_s[:, at], kf_s[:, at], qb_s[:, at], kb_s[:, at]
        value2, cot2 = both(value), both(cot)
        qf2, kf2, qb2, kb2 = both(qf), both(kf), both(qb), both(kb)
        d_score = nt(cot, value2)
        d_score_t = nt(value, cot2)
        score_t = jnp.where(upper, nt(kf, qf2), 0.0) + jnp.where(lower, nt(kb, qb2), 0.0)
        dqf_s[:, at] = nn(jnp.where(lower, d_score, 0.0).astype(BF16), kf2)
        dqb_s[:, at] = nn(jnp.where(upper, d_score, 0.0).astype(BF16), kb2)
        dkf_s[:, at] = nn(jnp.where(upper, d_score_t, 0.0).astype(BF16), qf2)
        dkb_s[:, at] = nn(jnp.where(lower, d_score_t, 0.0).astype(BF16), qb2)
        dv_s[:, at] = nn(score_t.astype(BF16), cot2)
        return 0

    def own_parts():
        lax.fori_loop(0, PAIRS, own_part, 0)

    @pl.when(z == 0)
    def _():
        recv_s[0] = jnp.zeros(recv_s.shape[1:], BF16)

    @pl.when(z == nz - 1)
    def _():
        recv_s[1] = jnp.zeros(recv_s.shape[1:], BF16)

    def chain_copy(way, j):
        return remote(
            send_s.at[way, j], recv_s.at[way, j], chain_ss.at[way, j], chain_rs.at[way, j],
            there(chip, c, lax.rem(z + 1 - 2 * way + nz, nz)),
        )

    def before(way):
        return z + way * (nz - 1 - 2 * z)

    def chain(way):
        def one(j, _):
            copy = chain_copy(way, j)

            @pl.when(before(way) > 0)
            def _():
                copy.wait_recv()

            @pl.when(before(way) < nz - 1)
            def _():
                end = end_s[0:1, lanes(lax.div(j, 2) * 128, 128)]
                state = recv_s[way, j].astype(F32) * end + loc_s[way, j]
                send_s[way, j] = state.astype(BF16)
                copy.start()

            return 0

        lax.fori_loop(0, CHUNKS, one, 0)

    first = lax.div(2 * z, nz)
    edge = jnp.minimum(z, nz - 1 - z)
    pl.when(edge >= 2)(own_parts)
    chain(first)
    pl.when(edge < 2)(own_parts)

    for copy in w1:
        copy.wait()
    w2 = []
    for i in range(1, nq):
        for j in range(nq):
            block = wv_s.at[c, chip_at(j, pb)]
            w2.append(
                remote(
                    block, block, w2_ss.at[(i - 1) * nq + j], w2_rs.at[(i - 1) * nq + j],
                    there(chip_at(pa, turned(pb, i, nq)), c),
                )
            )
    for copy in w2:
        copy.start()

    chain(1 - first)

    for copy in w2:
        copy.wait()
    w3 = remote(wv_s.at[c], wv_s.at[c], w3_ss, w3_rs, there(chip, 1 - c))
    w3.start()

    def spread(state):
        zero = jnp.zeros_like(state)
        return jnp.concatenate(
            [jnp.where(left_half, state, zero), jnp.where(left_half, zero, state)], axis=0
        ).astype(BF16)

    def finish(p, _):
        at = lanes(p * 128, 128)
        value = v_ref[:, at]
        cot = cot_ref[:, at]
        qf, kf, qb, kb = qf_s[:, at], kf_s[:, at], qb_s[:, at], kb_s[:, at]
        end = end_s[0:1, at]
        h_state = recv_s[0, 2 * p].astype(F32)
        f_state = recv_s[0, 2 * p + 1].astype(F32)
        e_state = (recv_s[1, 2 * p].astype(F32) * end).astype(BF16).astype(F32)
        r_state = (recv_s[1, 2 * p + 1].astype(F32) * end).astype(BF16).astype(F32)
        carry = jnp.sum(
            e_state * (h_state + raw_s[2 * p]) + r_state * (f_state + raw_s[2 * p + 1]),
            axis=0,
            keepdims=True,
        )
        h2, f2, e2, r2 = spread(h_state), spread(f_state), spread(e_state), spread(r_state)
        dqf = dqf_s[:, at] + nn(cot, h2)
        dqb = dqb_s[:, at] + nn(cot, r2)
        dkf = dkf_s[:, at] + nn(value, e2)
        dkb = dkb_s[:, at] + nn(value, f2)
        dvb_s[:, at] = (dv_s[:, at] + nt(kf, e2) + nt(kb, f2)).astype(BF16)
        running = run_s[:, at]
        exclusive = running - g_ref[:, at].astype(F32)
        dq = (jnp.exp(running) * dqf + jnp.exp(-exclusive) * dqb) * HEAD_DIM ** (-0.5)
        dk = jnp.exp(-running) * dkf + jnp.exp(exclusive) * dkb
        dq_ref[:, at] = dq.astype(BF16)
        dk_ref[:, at] = dk.astype(BF16)
        fwd = qf.astype(F32) * dqf - kf.astype(F32) * dkf
        bwd = kb.astype(F32) * dkb - qb.astype(F32) * dqb
        both_ways = fwd + bwd
        high = both_ways.astype(BF16)
        low = (both_ways - high.astype(F32)).astype(BF16)
        dg = nn(onward, high) + nn(onward, low) - bwd + carry
        dg_ref[:, at] = dg.astype(BF16)
        return 0

    lax.fori_loop(0, PAIRS, finish, 0)

    def send_dv(role, i):
        if role == 0:
            target = there(yy * nq + turned(xx, i, nq), 0)
        else:
            target = there(turned(yy, i, nq) * nq + xx, 1)
        src = dvb_s.at[:, pl.ds(role * HALF, HALF)]
        dst = dvg_s.at[x_slot[role]]

        def away():
            remote(src, dst, dv_ss.at[role, i], dv_rs.at[x_slot[role]], target).start()

        def at_home():
            pltpu.make_async_copy(src, dst, dv_rs.at[x_slot[role]]).start()

        if i == 0:
            pl.when(c != role)(away)
            pl.when(c == role)(at_home)
        else:
            away()

    for role in range(2):
        for i in range(nq):
            send_dv(role, i)

    w3.wait()
    group = nq * 128
    for i in range(nq):
        low_half = wv_s[0, i * nq : (i + 1) * nq].reshape(group, HALF)
        high_half = wv_s[1, i * nq : (i + 1) * nq].reshape(group, HALF)
        gi_ref[:, i * group : (i + 1) * group] = (
            nt(dvb_s[:, :HALF], low_half) + nt(dvb_s[:, HALF:], high_half)
        ).astype(BF16)

    for slot in range(2 * nq):
        remote(
            xg_s.at[slot], xg_s.at[slot], x_ss.at[0, 0], x_rs.at[slot], there(chip, 1 - c)
        ).wait_recv()
        remote(
            dvg_s.at[slot], dvg_s.at[slot], dv_ss.at[0, 0], dv_rs.at[slot], there(chip, 1 - c)
        ).wait_recv()
    tokens = 2 * nq * BLOCK
    all_dv = dvg_s[...].reshape(tokens, HALF)
    for b in range(nq):
        part = tn(xg_s[:, :, b * 128 : (b + 1) * 128].reshape(tokens, 128), all_dv)
        part_s[b] = part
        pb_s[b] = part.astype(BF16)

    s2 = [
        remote(
            pb_s.at[turned(pb, i, nq)], s2_s.at[i - 1], s2_ss.at[i - 1], s2_rs.at[i - 1],
            there(chip_at(pa, turned(pb, i, nq)), c),
        )
        for i in range(1, nq)
    ]
    for copy in s2:
        copy.start()
    total = part_s[pb]
    for i, copy in enumerate(s2):
        copy.wait()
        total = total + s2_s[i].astype(F32)
    acc_s[...] = total

    wide = nz // 4
    chunk = HALF // wide
    for j in range(nz):
        rows, columns = j // wide, j % wide
        zb_s[j] = acc_s[
            rows * 32 : (rows + 1) * 32, columns * chunk : (columns + 1) * chunk
        ].astype(BF16)

    def z_copy(i):
        to = turned(z, i, nz)
        return remote(
            zb_s.at[to], zr_s.at[i], zr_ss.at[i], zr_rs.at[i], there(chip, c, to)
        )

    def z_start(i, _):
        z_copy(i).start()
        return 0

    lax.fori_loop(1, nz, z_start, 0)

    def z_sum(i, summed):
        z_copy(i).wait()
        return summed + zr_s[i].astype(F32)

    summed = lax.fori_loop(1, nz, z_sum, zb_s[z].astype(F32))
    rb_s[...] = summed.astype(BF16)

    owner = lax.div(2 * z, nz)
    slot = c * (nz // 2) + lax.rem(z, nz // 2)

    def out_copy(i):
        return remote(
            rb_s, gr_s.at[slot], za_ss.at[i], za_rs.at[slot], there(chip, owner, turned(z, i, nz))
        )

    home = pltpu.make_async_copy(rb_s, gr_s.at[slot], za_rs.at[slot])
    pl.when(owner == c)(lambda: home.start())
    pl.when(owner != c)(lambda: out_copy(0).start())

    def out_start(i, _):
        out_copy(i).start()
        return 0

    lax.fori_loop(1, nz, out_start, 0)

    for role in range(2):
        for t in range(nz // 2):
            s = role * (nz // 2) + t
            remote(
                rb_s, gr_s.at[s], za_ss.at[0], za_rs.at[s], there(chip, 1 - c)
            ).wait_recv()
            rows, columns = t // wide, t % wide
            gw_ref[
                rows * 32 : (rows + 1) * 32,
                role * HALF + columns * chunk : role * HALF + (columns + 1) * chunk,
            ] = gr_s[s].astype(F32)

    pl.when(owner != c)(lambda: out_copy(0).wait_send())

    def out_sent(i, _):
        out_copy(i).wait_send()
        return 0

    lax.fori_loop(1, nz, out_sent, 0)

    for way in range(2):

        @pl.when(before(way) < nz - 1)
        def _():
            def sent(j, _):
                chain_copy(way, j).wait_send()
                return 0

            lax.fori_loop(0, CHUNKS, sent, 0)

    for role in range(2):
        for i in range(nq):

            def sent():
                remote(
                    xg_s.at[0], xg_s.at[0], x_ss.at[role, i], x_rs.at[0], there(chip, 1 - c)
                ).wait_send()
                remote(
                    dvg_s.at[0], dvg_s.at[0], dv_ss.at[role, i], dv_rs.at[0], there(chip, 1 - c)
                ).wait_send()

            if i == 0:
                pl.when(c != role)(sent)
            else:
                sent()


def per_device(nz, nq, inputs, queries, keys, values, log_decay, cotangent, value_weight):
    model = inputs.shape[2]
    slots = 2 * nq
    chunk = HALF // (nz // 4)
    dma = pltpu.SemaphoreType.DMA
    vm = pltpu.VMEM
    wide = jax.ShapeDtypeStruct((BLOCK, WIDTH), BF16)
    outs = pl.pallas_call(
        functools.partial(kernel, nz, nq),
        out_shape=(
            wide,
            wide,
            wide,
            jax.ShapeDtypeStruct((BLOCK, model), BF16),
            jax.ShapeDtypeStruct((64, WIDTH), F32),
        ),
        in_specs=[pl.BlockSpec(memory_space=pltpu.VMEM)] * 7,
        out_specs=[pl.BlockSpec(memory_space=pltpu.VMEM)] * 5,
        scratch_shapes=[
            vm((BLOCK, WIDTH), F32),
            vm((8, WIDTH), F32),
            *[vm((BLOCK, WIDTH), BF16)] * 4,
            vm((2, CHUNKS, 64, 128), F32),
            vm((CHUNKS, 64, 128), F32),
            vm((2, CHUNKS, 64, 128), BF16),
            vm((2, CHUNKS, 64, 128), BF16),
            *[vm((BLOCK, WIDTH), F32)] * 5,
            vm((BLOCK, WIDTH), BF16),
            vm((2, nq * nq, 128, HALF), BF16),
            vm((slots, BLOCK, nq * 128), BF16),
            vm((slots, BLOCK, HALF), BF16),
            vm((nq, 128, HALF), F32),
            vm((nq, 128, HALF), BF16),
            vm((nq - 1, 128, HALF), BF16),
            vm((128, HALF), F32),
            vm((nz, 32, chunk), BF16),
            vm((nz, 32, chunk), BF16),
            vm((32, chunk), BF16),
            vm((nz, 32, chunk), BF16),
            dma((2, CHUNKS)),
            dma((2, CHUNKS)),
            dma, dma, dma,
            dma((nq - 1,)), dma((nq - 1,)),
            dma(((nq - 1) * nq,)), dma(((nq - 1) * nq,)),
            dma, dma,
            dma((2, nq)), dma((slots,)),
            dma((2, nq)), dma((slots,)),
            dma((nq - 1,)), dma((nq - 1,)),
            dma((nz,)), dma((nz,)),
            dma((nz,)), dma((nz,)),
        ],
        compiler_params=pltpu.CompilerParams(
            collective_id=0, has_side_effects=True, vmem_limit_bytes=60 * 1024 * 1024
        ),
    )(
        queries[0], keys[0], values[0], log_decay[0], cotangent[0], inputs[0], value_weight
    )
    dq, dk, dg, gi, gw = outs
    return dq[None], dk[None], dg[None], gi[None], gw


def solution(mesh):
    nz = mesh.shape["sp"]
    nq = 4 if mesh.shape["dp"] == 32 else 2
    tokens = P("dp", "sp", None)
    return jax.shard_map(
        functools.partial(per_device, nz, nq),
        mesh=mesh,
        in_specs=(tokens,) * 6 + (P("dp", None),),
        out_specs=(tokens,) * 4 + (P("dp", None),),
        check_vma=False,
    )
```

```python
import functools

import jax
import jax.numpy as jnp
from jax import lax
from jax.experimental import pallas as pl
from jax.experimental.pallas import tpu as pltpu
from jax.sharding import PartitionSpec as P

MESH = pl.DeviceIdType.MESH
F32 = jnp.float32
BF16 = jnp.bfloat16
BLOCK = 128
WIDTH = 1024
HALF = WIDTH // 2
PAIRS = WIDTH // 128
CHUNKS = 2 * PAIRS
HEAD_DIM = 64


def nn(a, b):
    return lax.dot_general(a, b, (((1,), (0,)), ((), ())), preferred_element_type=F32)


def nt(a, b):
    return lax.dot_general(a, b, (((1,), (1,)), ((), ())), preferred_element_type=F32)


def tn(a, b):
    return lax.dot_general(a, b, (((0,), (0,)), ((), ())), preferred_element_type=F32)


def lanes(start, size):
    return pl.ds(pl.multiple_of(start, 128), size)


def kernel(
    nz, nq,
    q_ref, k_ref, v_ref, g_ref, cot_ref, x_ref, w_ref,
    dq_ref, dk_ref, dg_ref, gi_ref, gw_ref,
    run_s, end_s, qf_s, kf_s, qb_s, kb_s, loc_s, raw_s, send_s, recv_s,
    dqf_s, dqb_s, dkf_s, dkb_s, dv_s, dvb_s,
    wv_s, xg_s, xgt_s, dvg_s, part_s, pb_s, s2_s, zb_s, zr_s, rb_s, gr_s,
    chain_ss, chain_rs, fw_ss, fw_rs, loc_ss, loc_rs,
    w0_ss, w0_rs, w_loc, w1_ss, w1_rs, w2_ss, w2_rs, w3_ss, w3_rs,
    x_ss, x_rs, dv_ss, dv_rs, s2_ss, s2_rs, zr_ss, zr_rs, za_ss, za_rs,
):
    z = lax.axis_index("sp")
    d = lax.axis_index("dp")
    c = lax.rem(d, 2)
    chip = lax.div(d, 2)
    xx = lax.rem(chip, nq)
    yy = lax.div(chip, nq)
    pa = xx * (1 - c) + yy * c
    pb = yy * (1 - c) + xx * c

    def chip_at(a, b):
        return (b * nq + a) * (1 - c) + (a * nq + b) * c

    def there(chip_id, core, at_z=None):
        return {"sp": z if at_z is None else at_z, "dp": chip_id * 2 + core}

    def turned(at, i, n):
        return lax.rem(at + i, n)

    barrier = pltpu.get_barrier_semaphore()
    greeted = 0
    for i in range(1, nq):
        for core in range(2):
            for other in (yy * nq + turned(xx, i, nq), turned(yy, i, nq) * nq + xx):
                pl.semaphore_signal(barrier, inc=1, device_id=there(other, core), device_id_type=MESH)
                greeted += 1
    pl.semaphore_signal(barrier, inc=1, device_id=there(chip, 1 - c), device_id_type=MESH)
    for step in (1, nz - 1):
        pl.semaphore_signal(
            barrier, inc=1, device_id=there(chip, c, turned(z, step, nz)), device_id_type=MESH
        )
    def remote(src, dst, ss, rs, device):
        return pltpu.make_async_remote_copy(
            src_ref=src, dst_ref=dst, send_sem=ss, recv_sem=rs, device_id=device, device_id_type=MESH
        )

    row = lax.broadcasted_iota(jnp.int32, (BLOCK, BLOCK), 0)
    col = lax.broadcasted_iota(jnp.int32, (BLOCK, BLOCK), 1)
    left_half = lax.broadcasted_iota(jnp.int32, (64, 128), 1) < 64
    lane = lax.broadcasted_iota(jnp.int32, (BLOCK, 128), 1)
    mask0 = jnp.where(lane < 64, 1.0, 0.0).astype(BF16)
    mask1 = jnp.where(lane < 64, 0.0, 1.0).astype(BF16)
    upto = jnp.where(row >= col, 1.0, 0.0).astype(BF16)
    onward = jnp.where(row <= col, 1.0, 0.0).astype(BF16)

    def diagonal(m):
        return jnp.where(left_half, m[:64], m[64:])

    def local_states(p, _):
        at = lanes(p * 128, 128)
        gate = g_ref[:, at]
        running = nn(upto, gate)
        exclusive = running - gate.astype(F32)
        run_s[:, at] = running
        end = jnp.exp(running[BLOCK - 1 : BLOCK])
        end_s[1, :, at] = jnp.broadcast_to(end, (8, 128))
        query = q_ref[:, at].astype(F32) * HEAD_DIM ** (-0.5)
        key = k_ref[:, at].astype(F32)
        qf = (query * jnp.exp(running)).astype(BF16)
        kf = (key * jnp.exp(-running)).astype(BF16)
        qb = (query * jnp.exp(-exclusive)).astype(BF16)
        kb = (key * jnp.exp(exclusive)).astype(BF16)
        qf_s[:, at] = qf
        kf_s[:, at] = kf
        qb_s[:, at] = qb
        kb_s[:, at] = kb
        value = v_ref[:, at]
        cot = cot_ref[:, at]
        uh = diagonal(tn(value, kf))
        wb = diagonal(tn(cot, qb))
        raw_s[2 * p] = uh
        raw_s[2 * p + 1] = wb
        loc_s[1, p, 0, 0] = (uh * end).astype(BF16)
        loc_s[1, p, 0, 1] = (wb * end).astype(BF16)
        loc_s[1, p, 1, 0] = diagonal(tn(cot, qf)).astype(BF16)
        loc_s[1, p, 1, 1] = diagonal(tn(value, kb)).astype(BF16)
        return 0

    lax.fori_loop(0, PAIRS, local_states, 0)

    pl.semaphore_wait(barrier, greeted + 3)

    def state_copies():
        return (
            remote(loc_s.at[1], loc_s.at[0], loc_ss.at[0], loc_rs.at[0], there(chip, 1 - c)),
            remote(end_s.at[1], end_s.at[0], loc_ss.at[1], loc_rs.at[1], there(chip, 1 - c)),
        )

    @pl.when(c == 0)
    def _():
        for copy in state_copies():
            copy.start()

    w_here = pltpu.make_async_copy(
        w_ref.at[:, lanes(c * HALF, HALF)],
        wv_s.at[c, chip, pl.ds(pl.multiple_of(c * 64, 64), 64), :],
        w_loc,
    )
    w_here.start()
    w0 = remote(
        w_ref.at[:, lanes((1 - c) * HALF, HALF)],
        wv_s.at[1 - c, chip, pl.ds(pl.multiple_of(c * 64, 64), 64), :],
        w0_ss, w0_rs, there(chip, 1 - c),
    )
    w0.start()

    x_slot = (xx * 2 + c, yy * 2 + c)

    def x_copies(role, i):
        if role == 0:
            to = turned(xx, i, nq)
            target = there(yy * nq + to, 0)
            pieces = [
                (
                    x_ref.at[:, lanes((b * nq + to) * 128, 128)],
                    xg_s.at[x_slot[0], :, pl.ds(b * 128, 128)],
                )
                for b in range(nq)
            ]
        else:
            to = turned(yy, i, nq)
            target = there(to * nq + xx, 1)
            pieces = [(x_ref.at[:, lanes(to * nq * 128, nq * 128)], xg_s.at[x_slot[1]])]
        return target, pieces

    def send_x(role, i):
        target, pieces = x_copies(role, i)

        def away():
            for src, dst in pieces:
                remote(src, dst, x_ss.at[role, i], x_rs.at[x_slot[role]], target).start()

        def at_home():
            for src, dst in pieces:
                pltpu.make_async_copy(src, dst, x_rs.at[x_slot[role]]).start()

        if i == 0:
            pl.when(c != role)(away)
            pl.when(c == role)(at_home)
        else:
            away()

    for role in range(2):
        for i in range(nq):
            send_x(role, i)

    w_here.wait()
    w0.wait()
    w1 = [
        remote(
            wv_s.at[c, chip], wv_s.at[c, chip], w1_ss.at[i - 1], w1_rs.at[i - 1],
            there(chip_at(turned(pa, i, nq), pb), c),
        )
        for i in range(1, nq)
    ]
    for copy in w1:
        copy.start()

    def both(a):
        return jnp.concatenate([a * mask0, a * mask1], axis=0)

    row2 = lax.broadcasted_iota(jnp.int32, (BLOCK, 256), 0)
    col2 = lax.rem(lax.broadcasted_iota(jnp.int32, (BLOCK, 256), 1), 128)
    lower = row2 >= col2
    upper = row2 <= col2

    def own_part(p, _):
        at = lanes(p * 128, 128)
        value = v_ref[:, at]
        cot = cot_ref[:, at]
        qf, kf, qb, kb = qf_s[:, at], kf_s[:, at], qb_s[:, at], kb_s[:, at]
        value2, cot2 = both(value), both(cot)
        qf2, kf2, qb2, kb2 = both(qf), both(kf), both(qb), both(kb)
        d_score = nt(cot, value2)
        d_score_t = nt(value, cot2)
        score_t = jnp.where(upper, nt(kf, qf2), 0.0) + jnp.where(lower, nt(kb, qb2), 0.0)
        dqf_s[:, at] = nn(jnp.where(lower, d_score, 0.0).astype(BF16), kf2)
        dqb_s[:, at] = nn(jnp.where(upper, d_score, 0.0).astype(BF16), kb2)
        dkf_s[:, at] = nn(jnp.where(upper, d_score_t, 0.0).astype(BF16), qf2)
        dkb_s[:, at] = nn(jnp.where(lower, d_score_t, 0.0).astype(BF16), qb2)
        dv_s[:, at] = nn(score_t.astype(BF16), cot2)
        return 0

    def prepare():
        lax.fori_loop(0, PAIRS, own_part, 0)
        for slot in range(2 * nq):
            remote(
                xg_s.at[slot], xg_s.at[slot], x_ss.at[0, 0], x_rs.at[slot], there(chip, 1 - c)
            ).wait_recv()
            for b in range(nq):
                xgt_s[b, :, slot * BLOCK : (slot + 1) * BLOCK] = xg_s[
                    slot, :, b * 128 : (b + 1) * 128
                ].T

    def before(way):
        return z + way * (nz - 1 - 2 * z)

    for way in range(2):

        @pl.when(before(way) == 0)
        def _():
            recv_s[:, way] = jnp.zeros((2, *recv_s.shape[2:]), BF16)

    def chain_copy(s, way, j):
        return remote(
            send_s.at[s, way, j], recv_s.at[s, way, j],
            chain_ss.at[s, way, j], chain_rs.at[s, way, j],
            there(chip, c, lax.rem(z + 1 - 2 * way + nz, nz)),
        )

    def forward_copy(way, j):
        return remote(
            recv_s.at[0, way, j], recv_s.at[1, way, j],
            fw_ss.at[way, j], fw_rs.at[way, j], there(chip, 1 - c),
        )

    first = lax.div(2 * z, nz)
    edge = jnp.minimum(z, nz - 1 - z)
    steps = 2 * CHUNKS
    lead = 6
    lag = jnp.where(edge == nz // 2 - 1, 12, steps)

    def chain_step(t, _):
        turn = t - lag
        second = jnp.where(t < lag, 0, jnp.where(t < 2 * steps - lag, lax.rem(turn, 2), 1))
        index = jnp.where(
            t < lag,
            t,
            jnp.where(
                t < 2 * steps - lag,
                lax.div(turn, 2) + lag * (1 - lax.rem(turn, 2)),
                t - steps,
            ),
        )
        way = first + second - 2 * first * second
        theirs = jnp.where((index >= lead) & (index < lead + CHUNKS), 1, 0)
        s = 1 - theirs
        j = index - jnp.where(index < lead, 0, jnp.where(theirs == 1, lead, CHUNKS))
        copy = chain_copy(s, way, j)

        @pl.when(t == lead)
        def _():
            for taken in state_copies():
                taken.wait_recv()

        @pl.when(before(way) > 0)
        def _():
            copy.wait_recv()

            @pl.when(theirs == 1)
            def _():
                forward_copy(way, j).start()

        @pl.when(before(way) < nz - 1)
        def _():
            pair = lax.div(j, 2)
            end = end_s[s, 0:1, lanes(pair * 128, 128)]
            own = loc_s[s, pair, way, lax.rem(j, 2)].astype(F32)
            state = recv_s[s, way, j].astype(F32) * end + own
            send_s[s, way, j] = state.astype(BF16)
            copy.start()

        return 0

    early = edge >= nz // 4
    pl.when((c == 0) | early)(prepare)

    def chain(begin):
        @pl.when(c == 1)
        def _():
            lax.fori_loop(begin, begin + steps, chain_step, 0)

    chain(0)
    pl.when((c == 1) & (edge < nz // 4))(prepare)

    for copy in w1:
        copy.wait()
    w2 = []
    for i in range(1, nq):
        for j in range(nq):
            block = wv_s.at[c, chip_at(j, pb)]
            w2.append(
                remote(
                    block, block, w2_ss.at[(i - 1) * nq + j], w2_rs.at[(i - 1) * nq + j],
                    there(chip_at(pa, turned(pb, i, nq)), c),
                )
            )
    for copy in w2:
        copy.start()

    chain(steps)

    for copy in w2:
        copy.wait()
    w3 = remote(wv_s.at[c], wv_s.at[c], w3_ss, w3_rs, there(chip, 1 - c))
    w3.start()

    for way in range(2):

        @pl.when((c == 0) & (before(way) > 0))
        def _():
            def back(j, _):
                forward_copy(way, j).wait_recv()
                return 0

            lax.fori_loop(0, CHUNKS, back, 0)

    def spread(state):
        zero = jnp.zeros_like(state)
        return jnp.concatenate(
            [jnp.where(left_half, state, zero), jnp.where(left_half, zero, state)], axis=0
        ).astype(BF16)

    def value_part(i, _):
        p = lax.rem(i, 2) * (PAIRS // 2) + lax.div(i, 2)
        at = lanes(p * 128, 128)
        e2 = spread(recv_s[1, 1, 2 * p].astype(F32) * end_s[1, 0:1, at])
        f2 = spread(recv_s[1, 0, 2 * p + 1].astype(F32))
        dvb_s[:, at] = (dv_s[:, at] + nt(kf_s[:, at], e2) + nt(kb_s[:, at], f2)).astype(BF16)
        return 0

    def send_dv(h, role, i):
        if role == 0:
            target = there(yy * nq + turned(xx, i, nq), 0)
        else:
            target = there(turned(yy, i, nq) * nq + xx, 1)
        src = dvb_s.at[:, pl.ds(role * HALF + h * 256, 256)]
        dst = dvg_s.at[h, x_slot[role]]

        def away():
            remote(
                src, dst, dv_ss.at[h, role, i], dv_rs.at[h, x_slot[role]], target
            ).start()

        def at_home():
            pltpu.make_async_copy(src, dst, dv_rs.at[h, x_slot[role]]).start()

        if i == 0:
            pl.when(c != role)(away)
            pl.when(c == role)(at_home)
        else:
            away()

    for h in range(2):
        lax.fori_loop(h * (PAIRS // 2), (h + 1) * (PAIRS // 2), value_part, 0)
        for i in (2, 1, 3, 0) if nq == 4 else (1, 0):
            for role in range(2):
                send_dv(h, role, i)

    def finish(p, _):
        at = lanes(p * 128, 128)
        value = v_ref[:, at]
        cot = cot_ref[:, at]
        qf, kf, qb, kb = qf_s[:, at], kf_s[:, at], qb_s[:, at], kb_s[:, at]
        end = end_s[1, 0:1, at]
        h_state = recv_s[1, 0, 2 * p].astype(F32)
        f_state = recv_s[1, 0, 2 * p + 1].astype(F32)
        e_state = (recv_s[1, 1, 2 * p].astype(F32) * end).astype(BF16).astype(F32)
        r_state = (recv_s[1, 1, 2 * p + 1].astype(F32) * end).astype(BF16).astype(F32)
        carry = jnp.sum(
            e_state * (h_state + raw_s[2 * p]) + r_state * (f_state + raw_s[2 * p + 1]),
            axis=0,
            keepdims=True,
        )
        h2, f2, e2, r2 = spread(h_state), spread(f_state), spread(e_state), spread(r_state)
        dqf = dqf_s[:, at] + nn(cot, h2)
        dqb = dqb_s[:, at] + nn(cot, r2)
        dkf = dkf_s[:, at] + nn(value, e2)
        dkb = dkb_s[:, at] + nn(value, f2)
        running = run_s[:, at]
        exclusive = running - g_ref[:, at].astype(F32)
        dq = (jnp.exp(running) * dqf + jnp.exp(-exclusive) * dqb) * HEAD_DIM ** (-0.5)
        dk = jnp.exp(-running) * dkf + jnp.exp(exclusive) * dkb
        dq_ref[:, at] = dq.astype(BF16)
        dk_ref[:, at] = dk.astype(BF16)
        fwd = qf.astype(F32) * dqf - kf.astype(F32) * dkf
        bwd = kb.astype(F32) * dkb - qb.astype(F32) * dqb
        both_ways = fwd + bwd
        high = both_ways.astype(BF16)
        low = (both_ways - high.astype(F32)).astype(BF16)
        dg = nn(onward, high) + nn(onward, low) - bwd + carry
        dg_ref[:, at] = dg.astype(BF16)
        return 0

    lax.fori_loop(0, PAIRS, finish, 0)

    w3.wait()
    group = nq * 128
    for i in range(nq):
        low_half = wv_s[0, i * nq : (i + 1) * nq].reshape(group, HALF)
        high_half = wv_s[1, i * nq : (i + 1) * nq].reshape(group, HALF)
        gi_ref[:, i * group : (i + 1) * group] = (
            nt(dvb_s[:, :HALF], low_half) + nt(dvb_s[:, HALF:], high_half)
        ).astype(BF16)

    tokens = 2 * nq * BLOCK

    def s2_copies(h):
        return [
            remote(
                pb_s.at[h, turned(pb, i, nq)], s2_s.at[h, i - 1],
                s2_ss.at[h, i - 1], s2_rs.at[h, i - 1],
                there(chip_at(pa, turned(pb, i, nq)), c),
            )
            for i in range(1, nq)
        ]

    for h in range(2):
        for slot in range(2 * nq):
            remote(
                dvg_s.at[h, slot], dvg_s.at[h, slot], dv_ss.at[0, 0, 0], dv_rs.at[h, slot],
                there(chip, 1 - c),
            ).wait_recv()
        gathered = dvg_s[h].reshape(tokens, 256)
        for b in range(nq):
            part = nn(xgt_s[b], gathered)
            part_s[h, b] = part
            pb_s[h, b] = part.astype(BF16)
        for copy in s2_copies(h):
            copy.start()

    wide = 4 if nz == 16 else 2
    stack = nz // wide
    height = 128 // stack
    chunk = HALF // wide

    def z_copy(to):
        return remote(zb_s.at[to], zr_s.at[z], zr_ss.at[to], zr_rs.at[z], there(chip, c, to))

    for h in range(2):
        total = part_s[h, pb]
        for i, copy in enumerate(s2_copies(h)):
            copy.wait()
            total = total + s2_s[h, i].astype(F32)
        per = wide // 2
        for r in range(stack):
            for l in range(per):
                zb_s[r * wide + h * per + l] = total[
                    r * height : (r + 1) * height, l * chunk : (l + 1) * chunk
                ].astype(BF16)
        for r in (2, 1, 3, 0) if stack == 4 else (1, 0):
            group_at = lax.rem(lax.div(z, wide) + r, stack)
            for l in range(per):
                to = group_at * wide + h * per + l
                pl.when(to != z)(lambda: z_copy(to).start())

    zr_s[z] = zb_s[z]

    def z_wait(source, _):
        @pl.when(source != z)
        def _():
            remote(
                zb_s.at[source], zr_s.at[source], zr_ss.at[source], zr_rs.at[source],
                there(chip, c, source),
            ).wait()

        return 0

    lax.fori_loop(0, nz, z_wait, 0)
    rb_s[...] = jnp.sum(zr_s[...].astype(F32), axis=0).astype(BF16)

    owner = lax.div(2 * z, nz)
    slot = c * (nz // 2) + lax.rem(z, nz // 2)

    def out_copy(i):
        return remote(
            rb_s, gr_s.at[slot], za_ss.at[i], za_rs.at[slot], there(chip, owner, turned(z, i, nz))
        )

    home = pltpu.make_async_copy(rb_s, gr_s.at[slot], za_rs.at[slot])
    for near in range(nz // 2):
        out_copy(nz // 2 - near).start()
        if near > 0:
            out_copy(nz // 2 + near).start()
    pl.when(owner == c)(lambda: home.start())
    pl.when(owner != c)(lambda: out_copy(0).start())

    for role in range(2):
        for t in range(nz // 2):
            s = role * (nz // 2) + t
            remote(
                rb_s, gr_s.at[s], za_ss.at[0], za_rs.at[s], there(chip, 1 - c)
            ).wait_recv()
            rows, columns = t // wide, t % wide
            gw_ref[
                rows * height : (rows + 1) * height,
                role * HALF + columns * chunk : role * HALF + (columns + 1) * chunk,
            ] = gr_s[s].astype(F32)

    pl.when(owner != c)(lambda: out_copy(0).wait_send())

    def out_sent(i, _):
        out_copy(i).wait_send()
        return 0

    lax.fori_loop(1, nz, out_sent, 0)

    @pl.when(c == 0)
    def _():
        for copy in state_copies():
            copy.wait_send()

    for way in range(2):

        @pl.when((c == 1) & (before(way) < nz - 1))
        def _():
            def sent(j, _):
                for s in range(2):
                    chain_copy(s, way, j).wait_send()
                return 0

            lax.fori_loop(0, CHUNKS, sent, 0)

        @pl.when((c == 1) & (before(way) > 0))
        def _():
            def sent(j, _):
                forward_copy(way, j).wait_send()
                return 0

            lax.fori_loop(0, CHUNKS, sent, 0)

    for role in range(2):
        for i in range(nq):

            def sent():
                remote(
                    xg_s.at[0], xg_s.at[0], x_ss.at[role, i], x_rs.at[0], there(chip, 1 - c)
                ).wait_send()
                for h in range(2):
                    remote(
                        dvg_s.at[h, 0], dvg_s.at[h, 0], dv_ss.at[h, role, i], dv_rs.at[h, 0],
                        there(chip, 1 - c),
                    ).wait_send()

            if i == 0:
                pl.when(c != role)(sent)
            else:
                sent()


def store(*refs):
    count = len(refs) // 3
    sources, targets, sems = refs[:count], refs[count : 2 * count], refs[2 * count :]
    copies = [pltpu.make_async_copy(*each) for each in zip(sources, targets, sems)]
    for copy in copies:
        copy.start()
    for copy in copies:
        copy.wait()


def per_device(nz, nq, inputs, queries, keys, values, log_decay, cotangent, value_weight):
    model = inputs.shape[2]
    slots = 2 * nq
    wide = 4 if nz == 16 else 2
    chunk = (128 * wide // nz, HALF // wide)
    dma = pltpu.SemaphoreType.DMA
    vm = pltpu.VMEM
    shapes = [((BLOCK, WIDTH), BF16)] * 3 + [((BLOCK, model), BF16), ((64, WIDTH), F32)]
    in_vmem = pl.BlockSpec(memory_space=pltpu.VMEM)
    anywhere = pl.BlockSpec(memory_space=pl.ANY)
    outs = pl.pallas_call(
        functools.partial(kernel, nz, nq),
        out_shape=tuple(vm(*shape) for shape in shapes),
        in_specs=[in_vmem] * 5 + [anywhere] * 2,
        out_specs=[in_vmem] * 5,
        scratch_shapes=[
            vm((BLOCK, WIDTH), F32),
            vm((2, 8, WIDTH), F32),
            *[vm((BLOCK, WIDTH), BF16)] * 4,
            vm((2, PAIRS, 2, 2, 64, 128), BF16),
            vm((CHUNKS, 64, 128), F32),
            vm((2, 2, CHUNKS, 64, 128), BF16),
            vm((2, 2, CHUNKS, 64, 128), BF16),
            *[vm((BLOCK, WIDTH), F32)] * 5,
            vm((BLOCK, WIDTH), BF16),
            vm((2, nq * nq, 128, HALF), BF16),
            vm((slots, BLOCK, nq * 128), BF16),
            vm((nq, 128, slots * BLOCK), BF16),
            vm((2, slots, BLOCK, 256), BF16),
            vm((2, nq, 128, 256), F32),
            vm((2, nq, 128, 256), BF16),
            vm((2, nq - 1, 128, 256), BF16),
            vm((nz, *chunk), BF16),
            vm((nz, *chunk), BF16),
            vm(chunk, BF16),
            vm((nz, *chunk), BF16),
            dma((2, 2, CHUNKS)), dma((2, 2, CHUNKS)),
            dma((2, CHUNKS)), dma((2, CHUNKS)),
            dma((2,)), dma((2,)),
            dma, dma, dma,
            dma((nq - 1,)), dma((nq - 1,)),
            dma(((nq - 1) * nq,)), dma(((nq - 1) * nq,)),
            dma, dma,
            dma((2, nq)), dma((slots,)),
            dma((2, 2, nq)), dma((2, slots)),
            dma((2, nq - 1)), dma((2, nq - 1)),
            dma((nz,)), dma((nz,)),
            dma((nz,)), dma((nz,)),
        ],
        compiler_params=pltpu.CompilerParams(
            collective_id=0, has_side_effects=True, vmem_limit_bytes=65_300_000
        ),
    )(
        queries[0], keys[0], values[0], log_decay[0], cotangent[0], inputs[0], value_weight
    )
    dq, dk, dg, gi, gw = pl.pallas_call(
        store,
        out_shape=tuple(jax.ShapeDtypeStruct(*shape) for shape in shapes),
        in_specs=[anywhere] * 5,
        out_specs=[anywhere] * 5,
        scratch_shapes=[dma] * 5,
        compiler_params=pltpu.CompilerParams(vmem_limit_bytes=1024 * 1024),
    )(*outs)
    return dq[None], dk[None], dg[None], gi[None], gw


def solution(mesh):
    nz = mesh.shape["sp"]
    nq = 4 if mesh.shape["dp"] == 32 else 2
    tokens = P("dp", "sp", None)
    return jax.shard_map(
        functools.partial(per_device, nz, nq),
        mesh=mesh,
        in_specs=(tokens,) * 6 + (P("dp", None),),
        out_specs=(tokens,) * 4 + (P("dp", None),),
        check_vma=False,
    )
```

```python
import functools

import jax
import jax.numpy as jnp
from jax import lax
from jax.experimental import pallas as pl
from jax.experimental.pallas import tpu as pltpu
from jax.sharding import PartitionSpec as P

MESH = pl.DeviceIdType.MESH
F32 = jnp.float32
BF16 = jnp.bfloat16
BLOCK = 128
WIDTH = 1024
HALF = WIDTH // 2
PAIRS = WIDTH // 128
CHUNKS = 2 * PAIRS
HEAD_DIM = 64
UNROLL = 2


def nn(a, b):
    return lax.dot_general(a, b, (((1,), (0,)), ((), ())), preferred_element_type=F32)


def nt(a, b):
    return lax.dot_general(a, b, (((1,), (1,)), ((), ())), preferred_element_type=F32)


def tn(a, b):
    return lax.dot_general(a, b, (((0,), (0,)), ((), ())), preferred_element_type=F32)


def lanes(start, size):
    return pl.ds(pl.multiple_of(start, 128), size)


def kernel(
    nz, nq,
    q_in, k_in, v_in, g_in, cot_in, x_ref, w_ref,
    dq_out, dk_out, dg_out, gi_out, gr_s,
    q_ref, k_ref, v_ref, g_ref, cot_ref, dq_ref, dk_ref, dg_ref, gi_ref,
    run_s, end_s, qf_s, kf_s, qb_s, kb_s, loc_s, raw_s,
    fol_s, fend_s, in_s, out_s, state_s,
    dqf_s, dqb_s, dkf_s, dkb_s, dv_s, dvb_s,
    wv_s, xg_s, xgt_s, dvg_s, part_s, pb_s, s2_s, zb_s, zr_s, rb_s,
    in_sem, out_sem, chain_ss, chain_rs, hand_ss, hand_rs, fw_ss, fw_rs,
    loc_ss, loc_rs, fol_ss, fol_rs, fend_ss, fend_rs,
    w0_ss, w0_rs, w_loc, w1_ss, w1_rs, w2_ss, w2_rs, w3_ss, w3_rs,
    x_ss, x_rs, dv_ss, dv_rs, s2_ss, s2_rs, zr_ss, zr_rs, za_ss, za_rs,
):
    z = lax.axis_index("sp")
    d = lax.axis_index("dp")
    c = lax.rem(d, 2)
    chip = lax.div(d, 2)
    xx = lax.rem(chip, nq)
    yy = lax.div(chip, nq)
    pa = xx * (1 - c) + yy * c
    pb = yy * (1 - c) + xx * c

    def chip_at(a, b):
        return (b * nq + a) * (1 - c) + (a * nq + b) * c

    def there(chip_id, core, at_z=None):
        return {"sp": z if at_z is None else at_z, "dp": chip_id * 2 + core}

    def turned(at, i, n):
        return lax.rem(at + i, n)

    barrier = pltpu.get_barrier_semaphore()
    greeted = 0
    for i in range(1, nq):
        for core in range(2):
            for other in (yy * nq + turned(xx, i, nq), turned(yy, i, nq) * nq + xx):
                pl.semaphore_signal(barrier, inc=1, device_id=there(other, core), device_id_type=MESH)
                greeted += 1
    pl.semaphore_signal(barrier, inc=1, device_id=there(chip, 1 - c), device_id_type=MESH)
    mate = z + 1 - 2 * lax.rem(z, 2)
    for at_z, core in (
        (mate, 0), (mate, 1), (turned(z, 2, nz), c), (turned(z, nz - 2, nz), c)
    ):
        pl.semaphore_signal(
            barrier, inc=1, device_id=there(chip, core, at_z), device_id_type=MESH
        )

    def left(ref, sem):
        remote(ref, ref, sem, sem, there(chip, 1 - c)).wait_send()

    def arrived(ref, sem):
        remote(ref, ref, sem, sem, there(chip, 1 - c)).wait_recv()

    inputs = []
    for h in range(2):
        half = pl.ds(h * HALF, HALF)
        inputs.append(
            [
                pltpu.make_async_copy(a.at[:, half], b.at[:, half], in_sem.at[h, n])
                for n, (a, b) in enumerate(
                    (
                        (g_in, g_ref), (q_in, q_ref), (k_in, k_ref),
                        (v_in, v_ref), (cot_in, cot_ref),
                    )
                )
            ]
        )
    for copies in inputs:
        for copy in copies:
            copy.start()

    def remote(src, dst, ss, rs, device):
        return pltpu.make_async_remote_copy(
            src_ref=src, dst_ref=dst, send_sem=ss, recv_sem=rs, device_id=device, device_id_type=MESH
        )

    row = lax.broadcasted_iota(jnp.int32, (BLOCK, BLOCK), 0)
    col = lax.broadcasted_iota(jnp.int32, (BLOCK, BLOCK), 1)
    left_half = lax.broadcasted_iota(jnp.int32, (64, 128), 1) < 64
    lane = lax.broadcasted_iota(jnp.int32, (BLOCK, 128), 1)
    mask0 = jnp.where(lane < 64, 1.0, 0.0).astype(BF16)
    mask1 = jnp.where(lane < 64, 0.0, 1.0).astype(BF16)
    upto = jnp.where(row >= col, 1.0, 0.0).astype(BF16)
    onward = jnp.where(row <= col, 1.0, 0.0).astype(BF16)

    def diagonal(m):
        return jnp.where(left_half, m[:64], m[64:])

    def pair_at(k):
        return lax.rem(k, 2) + 4 * lax.rem(lax.div(k, 2), 2) + 2 * lax.div(k, 4)

    def local_states(p, _):
        at = lanes(p * 128, 128)
        gate = g_ref[:, at]
        running = nn(upto, gate)
        exclusive = running - gate.astype(F32)
        run_s[:, at] = running
        end = jnp.exp(running[BLOCK - 1 : BLOCK])
        end_s[1, :, at] = jnp.broadcast_to(end, (8, 128))
        query = q_ref[:, at].astype(F32) * HEAD_DIM ** (-0.5)
        key = k_ref[:, at].astype(F32)
        qf = (query * jnp.exp(running)).astype(BF16)
        kf = (key * jnp.exp(-running)).astype(BF16)
        qb = (query * jnp.exp(-exclusive)).astype(BF16)
        kb = (key * jnp.exp(exclusive)).astype(BF16)
        qf_s[:, at] = qf
        kf_s[:, at] = kf
        qb_s[:, at] = qb
        kb_s[:, at] = kb
        value = v_ref[:, at]
        cot = cot_ref[:, at]
        uh = diagonal(tn(value, kf))
        wb = diagonal(tn(cot, qb))
        raw_s[2 * p] = uh
        raw_s[2 * p + 1] = wb
        place = 2 * pair_at(p)
        loc_s[1, 0, place] = (uh * end).astype(BF16)
        loc_s[1, 0, place + 1] = (wb * end).astype(BF16)
        loc_s[1, 1, place] = diagonal(tn(cot, qf)).astype(BF16)
        loc_s[1, 1, place + 1] = diagonal(tn(value, kb)).astype(BF16)
        return 0

    for h, copies in enumerate(inputs):
        for copy in copies:
            copy.wait()
        lax.fori_loop(h * (PAIRS // 2), (h + 1) * (PAIRS // 2), local_states, 0, unroll=UNROLL)

    pl.semaphore_wait(barrier, greeted + 5)

    lead = 1 - lax.rem(z, 2)
    follow = 1 - lead
    quarter = CHUNKS // 4

    def state_copies():
        return (
            remote(loc_s.at[1, lead], loc_s.at[0, lead], loc_ss.at[0], loc_rs.at[0], there(chip, 1 - c)),
            remote(end_s.at[1], end_s.at[0], loc_ss.at[1], loc_rs.at[1], there(chip, 1 - c)),
        )

    remote(
        end_s.at[1], fend_s.at[c], fend_ss, fend_rs.at[c], there(chip, 1, mate)
    ).start()
    for n in range(4):
        part = pl.ds(n * quarter, quarter)
        remote(
            loc_s.at[1, follow, part], fol_s.at[c, part], fol_ss, fol_rs.at[c, n],
            there(chip, 1, mate),
        ).start()

    @pl.when(c == 0)
    def _():
        for copy in state_copies():
            copy.start()

    for half in range(2):
        columns = pl.ds(half * HALF, HALF)
        mine = wv_s.at[half, chip, pl.ds(pl.multiple_of(c * 64, 64), 64), :]

        @pl.when(c == 0)
        def _():
            pltpu.make_async_copy(w_ref.at[:, columns], mine, w_loc).start()

        @pl.when(c == 1)
        def _():
            remote(w_ref.at[:, columns], mine, w0_ss, w0_rs, there(chip, 0)).start()

    w_shard = wv_s.at[:, chip, pl.ds(0, 64), :]

    x_slot = (xx * 2 + c, yy * 2 + c)

    def x_copies(role, i):
        if role == 0:
            to = turned(xx, i, nq)
            target = there(yy * nq + to, 0)
            pieces = [
                (
                    x_ref.at[:, lanes((b * nq + to) * 128, 128)],
                    xg_s.at[x_slot[0], :, pl.ds(b * 128, 128)],
                )
                for b in range(nq)
            ]
        else:
            to = turned(yy, i, nq)
            target = there(to * nq + xx, 1)
            pieces = [(x_ref.at[:, lanes(to * nq * 128, nq * 128)], xg_s.at[x_slot[1]])]
        return target, pieces

    def send_x(role, i):
        target, pieces = x_copies(role, i)

        def away():
            for src, dst in pieces:
                remote(src, dst, x_ss, x_rs, target).start()

        def at_home():
            for src, dst in pieces:
                pltpu.make_async_copy(src, dst, x_rs).start()

        if i == 0:
            pl.when(c != role)(away)
            pl.when(c == role)(at_home)
        else:
            away()

    for role in range(2):
        for i in range(nq):
            send_x(role, i)

    def chip_in(half, a, b):
        return b * nq + a if half == 0 else a * nq + b

    w_at = ((xx, yy), (yy, xx))

    def w_first():
        pltpu.make_async_copy(w_shard, w_shard, w_loc).wait()
        arrived(w_shard, w0_rs)
        for half, (a, b) in enumerate(w_at):
            for i in range(1, nq):
                remote(
                    wv_s.at[half, chip], wv_s.at[half, chip], w1_ss, w1_rs.at[half],
                    there(chip_in(half, turned(a, i, nq), b), 0),
                ).start()

    def both(a):
        return jnp.concatenate([a * mask0, a * mask1], axis=0)

    row2 = lax.broadcasted_iota(jnp.int32, (BLOCK, 256), 0)
    col2 = lax.rem(lax.broadcasted_iota(jnp.int32, (BLOCK, 256), 1), 128)
    lower = row2 >= col2
    upper = row2 <= col2

    def own_part(p, _):
        at = lanes(p * 128, 128)
        value = v_ref[:, at]
        cot = cot_ref[:, at]
        qf, kf, qb, kb = qf_s[:, at], kf_s[:, at], qb_s[:, at], kb_s[:, at]
        value2, cot2 = both(value), both(cot)
        qf2, kf2, qb2, kb2 = both(qf), both(kf), both(qb), both(kb)
        d_score = nt(cot, value2)
        d_score_t = nt(value, cot2)
        score_t = jnp.where(upper, nt(kf, qf2), 0.0) + jnp.where(lower, nt(kb, qb2), 0.0)
        dqf_s[:, at] = nn(jnp.where(lower, d_score, 0.0).astype(BF16), kf2)
        dqb_s[:, at] = nn(jnp.where(upper, d_score, 0.0).astype(BF16), kb2)
        dkf_s[:, at] = nn(jnp.where(upper, d_score_t, 0.0).astype(BF16), qf2)
        dkb_s[:, at] = nn(jnp.where(lower, d_score_t, 0.0).astype(BF16), qb2)
        dv_s[:, at] = nn(score_t.astype(BF16), cot2)
        return 0

    def own_parts():
        lax.fori_loop(0, PAIRS, own_part, 0, unroll=UNROLL)

    def turn_inputs():
        arrived(xg_s, x_rs)
        for slot in range(2 * nq):
            for b in range(nq):
                xgt_s[b, :, slot * BLOCK : (slot + 1) * BLOCK] = xg_s[
                    slot, :, b * 128 : (b + 1) * 128
                ].T

    def w_second():
        for half, (a, b) in enumerate(w_at):
            arrived(wv_s.at[0, pl.ds(0, nq - 1)], w1_rs.at[half])
            for i in range(1, nq):
                for j in range(nq):
                    block = wv_s.at[half, chip_in(half, j, b)]
                    remote(
                        block, block, w2_ss, w2_rs,
                        there(chip_in(half, a, turned(b, i, nq)), 0),
                    ).start()

    def before(way):
        return z + way * (nz - 1 - 2 * z)

    for way in range(2):

        @pl.when(before(way) == 0)
        def _():
            state_s[:, way] = jnp.zeros((2, *state_s.shape[2:]), BF16)

    @pl.when(before(lead) == 1)
    def _():
        in_s[...] = jnp.zeros(in_s.shape, BF16)

    def onward_copy(s, i):
        return remote(
            out_s.at[s, i], in_s.at[s, i], chain_ss.at[s], chain_rs.at[s, i],
            there(chip, 1, lax.rem(z + 2 - 4 * lead + nz, nz)),
        )

    def hand_copy(s, i, way):
        return remote(
            in_s.at[s, i], state_s.at[s, way, i], hand_ss.at[s], hand_rs.at[s, i],
            there(chip, 1, mate),
        )

    def forward_copy(way, i):
        return remote(
            state_s.at[0, way, i], state_s.at[1, way, i],
            fw_ss.at[way], fw_rs.at[lax.div(i, CHUNKS // 2), way], there(chip, 1 - c),
        )

    edge = jnp.minimum(z, nz - 1 - z)
    first = jnp.where(edge >= nz // 4, lead, lax.div(2 * z, nz))
    steps = 2 * CHUNKS
    own_first = CHUNKS // 2

    def taken(index):
        theirs = jnp.where((index >= own_first) & (index < own_first + CHUNKS), 1, 0)
        i = index - jnp.where(index < own_first, 0, jnp.where(theirs == 1, own_first, CHUNKS))
        return 1 - theirs, i

    def lead_step(index, _):
        s, i = taken(index)
        onward = onward_copy(s, i)

        @pl.when(index == 0)
        def _():
            arrived(fend_s.at[1], fend_rs.at[1])

        @pl.when(index == own_first)
        def _():
            arrived(fend_s.at[0], fend_rs.at[0])
            for copy in state_copies():
                copy.wait_recv()

        @pl.when(lax.rem(i, quarter) == 0)
        def _():
            arrived(fol_s.at[0, pl.ds(0, quarter)], fol_rs.at[s, lax.div(i, quarter)])

        @pl.when(before(lead) > 1)
        def _():
            onward.wait_recv()

        at = lanes(pair_at(lax.div(i, 2)) * 128, 128)
        state = in_s[s, i].astype(F32) * fend_s[s, 0:1, at] + fol_s[s, i].astype(F32)
        state_s[s, lead, i] = state.astype(BF16)

        @pl.when(before(lead) < nz - 1)
        def _():
            behind = state * end_s[s, 0:1, at] + loc_s[s, lead, i].astype(F32)
            out_s[s, i] = behind.astype(BF16)
            onward.start()

        @pl.when(before(lead) > 1)
        def _():
            hand_copy(s, i, lead).start()

        @pl.when(s == 0)
        def _():
            forward_copy(lead, i).start()

        return 0

    def follow_step(index, _):
        s, i = taken(index)
        hand_copy(s, i, follow).wait_recv()

        @pl.when(s == 0)
        def _():
            forward_copy(follow, i).start()

        return 0

    def chain(way, begin, end):
        @pl.when((c == 1) & (way == lead))
        def _():
            lax.fori_loop(begin, end, lead_step, 0)

        @pl.when((c == 1) & (way != lead) & (before(follow) > 0))
        def _():
            lax.fori_loop(begin, end, follow_step, 0)

    pl.when(c == 0)(w_first)
    pl.when((c == 0) | (edge >= nz // 4))(own_parts)
    chain(first, 0, steps)
    pl.when((c == 1) & (edge < nz // 4))(own_parts)
    pl.when(c == 0)(w_second)
    pl.when((c == 0) | (edge < 2))(turn_inputs)

    def spread(state):
        zero = jnp.zeros_like(state)
        return jnp.concatenate(
            [jnp.where(left_half, state, zero), jnp.where(left_half, zero, state)], axis=0
        ).astype(BF16)

    def value_part(i, _):
        p = pair_at(i)
        at = lanes(p * 128, 128)
        e2 = spread(state_s[1, 1, 2 * i].astype(F32) * end_s[1, 0:1, at])
        f2 = spread(state_s[1, 0, 2 * i + 1].astype(F32))
        dvb_s[:, at] = (dv_s[:, at] + nt(kf_s[:, at], e2) + nt(kb_s[:, at], f2)).astype(BF16)
        return 0

    def w_swap():
        arrived(wv_s.at[:, pl.ds(0, (nq - 1) * nq)], w2_rs)
        remote(wv_s, wv_s, w3_ss, w3_rs, there(chip, 1)).start()

    def send_dv(h, role, i):
        if role == 0:
            target = there(yy * nq + turned(xx, i, nq), 0)
        else:
            target = there(turned(yy, i, nq) * nq + xx, 1)
        src = dvb_s.at[:, pl.ds(role * HALF + h * 256, 256)]
        dst = dvg_s.at[h, x_slot[role]]

        def away():
            remote(src, dst, dv_ss, dv_rs.at[h], target).start()

        def at_home():
            pltpu.make_async_copy(src, dst, dv_rs.at[h]).start()

        if i == 0:
            pl.when(c != role)(away)
            pl.when(c == role)(at_home)
        else:
            away()

    def back(h):
        for way in range(2):

            @pl.when((c == 0) & (before(way) > 0))
            def _():
                arrived(state_s.at[1, way, pl.ds(0, CHUNKS // 2)], fw_rs.at[h, way])

    for h in range(2):
        chain(1 - first, h * CHUNKS, (h + 1) * CHUNKS)
        back(h)
        lax.fori_loop(
            h * (PAIRS // 2), (h + 1) * (PAIRS // 2), value_part, 0, unroll=UNROLL
        )
        for i in (2, 1, 3, 0) if nq == 4 else (1, 0):
            for role in range(2):
                send_dv(h, role, i)

    def finish(p, _):
        at = lanes(p * 128, 128)
        value = v_ref[:, at]
        cot = cot_ref[:, at]
        qf, kf, qb, kb = qf_s[:, at], kf_s[:, at], qb_s[:, at], kb_s[:, at]
        end = end_s[1, 0:1, at]
        place = 2 * pair_at(p)
        h_state = state_s[1, 0, place].astype(F32)
        f_state = state_s[1, 0, place + 1].astype(F32)
        e_state = (state_s[1, 1, place].astype(F32) * end).astype(BF16).astype(F32)
        r_state = (state_s[1, 1, place + 1].astype(F32) * end).astype(BF16).astype(F32)
        carry = jnp.sum(
            e_state * (h_state + raw_s[2 * p]) + r_state * (f_state + raw_s[2 * p + 1]),
            axis=0,
            keepdims=True,
        )
        h2, f2, e2, r2 = spread(h_state), spread(f_state), spread(e_state), spread(r_state)
        dqf = dqf_s[:, at] + nn(cot, h2)
        dqb = dqb_s[:, at] + nn(cot, r2)
        dkf = dkf_s[:, at] + nn(value, e2)
        dkb = dkb_s[:, at] + nn(value, f2)
        running = run_s[:, at]
        exclusive = running - g_ref[:, at].astype(F32)
        dq = (jnp.exp(running) * dqf + jnp.exp(-exclusive) * dqb) * HEAD_DIM ** (-0.5)
        dk = jnp.exp(-running) * dkf + jnp.exp(exclusive) * dkb
        dq_ref[:, at] = dq.astype(BF16)
        dk_ref[:, at] = dk.astype(BF16)
        fwd = qf.astype(F32) * dqf - kf.astype(F32) * dkf
        bwd = kb.astype(F32) * dkb - qb.astype(F32) * dqb
        both_ways = fwd + bwd
        high = both_ways.astype(BF16)
        low = (both_ways - high.astype(F32)).astype(BF16)
        dg = nn(onward, high) + nn(onward, low) - bwd + carry
        dg_ref[:, at] = dg.astype(BF16)
        return 0

    pl.when((c == 1) & (edge >= 2))(turn_inputs)
    pl.when(c == 0)(w_swap)
    lax.fori_loop(0, PAIRS, finish, 0, unroll=UNROLL)

    outputs = [
        pltpu.make_async_copy(a, b, out_sem.at[n])
        for n, (a, b) in enumerate(
            ((dq_ref, dq_out), (dk_ref, dk_out), (dg_ref, dg_out), (gi_ref, gi_out))
        )
    ]
    for copy in outputs[:3]:
        copy.start()

    tokens = 2 * nq * BLOCK

    def s2_copies(h):
        return [
            remote(
                pb_s.at[h, turned(pb, i, nq)], s2_s.at[h, i - 1],
                s2_ss.at[h], s2_rs.at[h],
                there(chip_at(pa, turned(pb, i, nq)), c),
            )
            for i in range(1, nq)
        ]

    for h in range(2):
        arrived(dvg_s.at[h], dv_rs.at[h])
        gathered = dvg_s[h].reshape(tokens, 256)
        for b in range(nq):
            part = nn(xgt_s[b], gathered)
            part_s[h, b] = part
            pb_s[h, b] = part.astype(BF16)
        for copy in s2_copies(h):
            copy.start()

    wide = 4 if nz == 16 else 2
    stack = nz // wide
    height = 128 // stack
    chunk = HALF // wide

    def z_copy(to):
        return remote(zb_s.at[to], zr_s.at[z], zr_ss, zr_rs, there(chip, c, to))

    for h in range(2):
        total = part_s[h, pb]
        left(s2_s.at[h], s2_ss.at[h])
        arrived(s2_s.at[h], s2_rs.at[h])
        for i in range(nq - 1):
            total = total + s2_s[h, i].astype(F32)
        per = wide // 2
        for r in range(stack):
            for l in range(per):
                zb_s[r * wide + h * per + l] = total[
                    r * height : (r + 1) * height, l * chunk : (l + 1) * chunk
                ].astype(BF16)
        for r in (2, 1, 3, 0) if stack == 4 else (1, 0):
            group_at = lax.rem(lax.div(z, wide) + r, stack)
            for l in range(per):
                to = group_at * wide + h * per + l
                pl.when(to != z)(lambda: z_copy(to).start())

    zr_s[z] = zb_s[z]

    left(zr_s.at[pl.ds(0, nz - 1)], zr_ss)
    arrived(zr_s.at[pl.ds(0, nz - 1)], zr_rs)
    rb_s[...] = jnp.sum(zr_s[...].astype(F32), axis=0).astype(BF16)

    owner = lax.div(2 * z, nz)
    slot = c * (nz // 2) + lax.rem(z, nz // 2)

    def out_copy(i):
        return remote(
            rb_s, gr_s.at[slot], za_ss, za_rs, there(chip, owner, turned(z, i, nz))
        )

    home = pltpu.make_async_copy(rb_s, gr_s.at[slot], za_rs)
    for near in range(nz // 2):
        out_copy(nz // 2 - near).start()
        if near > 0:
            out_copy(nz // 2 + near).start()
    pl.when(owner == c)(lambda: home.start())
    pl.when(owner != c)(lambda: out_copy(0).start())

    pl.when(c == 1)(lambda: arrived(wv_s, w3_rs))
    group = nq * 128
    for i in range(nq):
        low_half = wv_s[0, i * nq : (i + 1) * nq].reshape(group, HALF)
        high_half = wv_s[1, i * nq : (i + 1) * nq].reshape(group, HALF)
        gi_ref[:, i * group : (i + 1) * group] = (
            nt(dvb_s[:, :HALF], low_half) + nt(dvb_s[:, HALF:], high_half)
        ).astype(BF16)

    outputs[3].start()

    arrived(gr_s, za_rs)

    for copy in outputs:
        copy.wait()
    pl.when(owner == c)(lambda: left(zr_s.at[pl.ds(0, nz - 1)], za_ss))
    pl.when(owner != c)(lambda: left(zr_s, za_ss))

    @pl.when(c == 0)
    def _():
        for copy in state_copies():
            copy.wait_send()

    left(end_s.at[1], fend_ss)
    left(fol_s.at[0], fol_ss)

    @pl.when((c == 1) & (before(lead) < nz - 1))
    def _():
        for s in range(2):
            left(out_s.at[s], chain_ss.at[s])

    @pl.when((c == 1) & (before(lead) > 1))
    def _():
        for s in range(2):
            left(in_s.at[s], hand_ss.at[s])

    for way in range(2):

        @pl.when((c == 1) & (before(way) > 0))
        def _():
            left(state_s.at[0, way], fw_ss.at[way])

    @pl.when(c == 0)
    def _():
        left(wv_s.at[:, pl.ds(0, nq - 1)], w1_ss)
        left(wv_s.at[:, pl.ds(0, (nq - 1) * nq)], w2_ss)
        left(wv_s, w3_ss)

    @pl.when(c == 1)
    def _():
        left(w_shard, w0_ss)

    left(xg_s.at[pl.ds(0, 2 * nq - 1)], x_ss)
    left(dvg_s.at[:, pl.ds(0, 2 * nq - 1)], dv_ss)


def store(wide, dq, dk, dg, gi, gr, dq_out, dk_out, dg_out, gi_out, gw_out, gw_s, sems):
    copies = [
        pltpu.make_async_copy(a, b, sems.at[n])
        for n, (a, b) in enumerate(((gi, gi_out), (dq, dq_out), (dk, dk_out), (dg, dg_out)))
    ]
    for copy in copies:
        copy.start()
    count, height, chunk = gr.shape
    for s in range(count):
        role, t = s // (count // 2), s % (count // 2)
        rows, columns = t // wide * height, role * HALF + t % wide * chunk
        gw_s[rows : rows + height, columns : columns + chunk] = gr[s].astype(F32)
    last = pltpu.make_async_copy(gw_s, gw_out, sems.at[4])
    last.start()
    for copy in (*copies, last):
        copy.wait()


def per_device(nz, nq, inputs, queries, keys, values, log_decay, cotangent, value_weight):
    model = inputs.shape[2]
    slots = 2 * nq
    wide = 4 if nz == 16 else 2
    chunk = (128 * wide // nz, HALF // wide)
    dma = pltpu.SemaphoreType.DMA
    vm = pltpu.VMEM
    shapes = [((BLOCK, WIDTH), BF16)] * 3 + [((BLOCK, model), BF16)]
    sums = ((nz, *chunk), BF16)
    weight = ((64, WIDTH), F32)
    in_vmem = pl.BlockSpec(memory_space=pltpu.VMEM)
    anywhere = pl.BlockSpec(memory_space=pl.ANY)
    outs = pl.pallas_call(
        functools.partial(kernel, nz, nq),
        out_shape=tuple(vm(*shape) for shape in (*shapes, sums)),
        in_specs=[anywhere] * 7,
        out_specs=[anywhere] * 5,
        scratch_shapes=[
            *[vm((BLOCK, WIDTH), BF16)] * 8,
            vm((BLOCK, model), BF16),
            vm((BLOCK, WIDTH), F32),
            vm((2, 8, WIDTH), F32),
            *[vm((BLOCK, WIDTH), BF16)] * 4,
            vm((2, 2, CHUNKS, 64, 128), BF16),
            vm((CHUNKS, 64, 128), F32),
            vm((2, CHUNKS, 64, 128), BF16),
            vm((2, 8, WIDTH), F32),
            vm((2, CHUNKS, 64, 128), BF16),
            vm((2, CHUNKS, 64, 128), BF16),
            vm((2, 2, CHUNKS, 64, 128), BF16),
            *[vm((BLOCK, WIDTH), F32)] * 5,
            vm((BLOCK, WIDTH), BF16),
            vm((2, nq * nq, 128, HALF), BF16),
            vm((slots, BLOCK, nq * 128), BF16),
            vm((nq, 128, slots * BLOCK), BF16),
            vm((2, slots, BLOCK, 256), BF16),
            vm((2, nq, 128, 256), F32),
            vm((2, nq, 128, 256), BF16),
            vm((2, nq - 1, 128, 256), BF16),
            vm(*sums),
            vm(*sums),
            vm(chunk, BF16),
            dma((2, 5)), dma((4,)),
            dma((2,)), dma((2, CHUNKS)),
            dma((2,)), dma((2, CHUNKS)),
            dma((2,)), dma((2, 2)),
            dma((2,)), dma((2,)),
            dma, dma((2, 4)),
            dma, dma((2,)),
            *[dma] * 4,
            dma((2,)),
            *[dma] * 7,
            dma((2,)),
            dma((2,)), dma((2,)),
            *[dma] * 4,
        ],
        compiler_params=pltpu.CompilerParams(
            collective_id=0, has_side_effects=True, vmem_limit_bytes=65_300_000
        ),
    )(
        queries[0], keys[0], values[0], log_decay[0], cotangent[0], inputs[0], value_weight
    )
    dq, dk, dg, gi, gw = pl.pallas_call(
        functools.partial(store, wide),
        out_shape=tuple(jax.ShapeDtypeStruct(*shape) for shape in (*shapes, weight)),
        in_specs=[anywhere] * 4 + [in_vmem],
        out_specs=[anywhere] * 5,
        scratch_shapes=[vm(*weight), dma((5,))],
        compiler_params=pltpu.CompilerParams(vmem_limit_bytes=1024 * 1024),
    )(*outs)
    return dq[None], dk[None], dg[None], gi[None], gw


def solution(mesh):
    nz = mesh.shape["sp"]
    nq = 4 if mesh.shape["dp"] == 32 else 2
    tokens = P("dp", "sp", None)
    return jax.shard_map(
        functools.partial(per_device, nz, nq),
        mesh=mesh,
        in_specs=(tokens,) * 6 + (P("dp", None),),
        out_specs=(tokens,) * 4 + (P("dp", None),),
        check_vma=False,
    )
```

```python
import functools

import jax
import jax.numpy as jnp
from jax import lax
from jax.experimental import pallas as pl
from jax.experimental.pallas import tpu as pltpu
from jax.sharding import PartitionSpec as P

MESH = pl.DeviceIdType.MESH
F32 = jnp.float32
BF16 = jnp.bfloat16
BLOCK = 128
WIDTH = 1024
HALF = WIDTH // 2
PAIRS = WIDTH // 128
CHUNKS = 2 * PAIRS
HEAD_DIM = 64
UNROLL = 2
PARTS = 4


def nn(a, b):
    return lax.dot_general(a, b, (((1,), (0,)), ((), ())), preferred_element_type=F32)


def nt(a, b):
    return lax.dot_general(a, b, (((1,), (1,)), ((), ())), preferred_element_type=F32)


def tn(a, b):
    return lax.dot_general(a, b, (((0,), (0,)), ((), ())), preferred_element_type=F32)


def lanes(start, size):
    return pl.ds(pl.multiple_of(start, 128), size)


def kernel(
    nz, nq,
    q_in, k_in, v_in, g_in, cot_in, x_ref, w_ref,
    dq_out, dk_out, dg_out, gi_out, gr_s,
    q_ref, k_ref, v_ref, g_ref, cot_ref, dq_ref, dk_ref, dg_ref, gi_ref,
    run_s, end_s, qf_s, kf_s, qb_s, kb_s, loc_s, raw_s,
    fol_s, fend_s, in_s, out_s, state_s,
    dqf_s, dqb_s, dkf_s, dkb_s, dv_s, dvb_s,
    wv_s, xg_s, xgt_s, dvg_s, part_s, pb_s, s2_s, zb_s, zr_s, rb_s,
    in_sem, out_sem, chain_ss, chain_rs, hand_ss, hand_rs, fw_ss, fw_rs,
    loc_ss, loc_rs, fol_ss, fol_rs, fend_ss, fend_rs,
    w0_ss, w0_rs, w_loc, w1_ss, w1_rs, w2_ss, w2_rs, w3_ss, w3_rs,
    x_ss, x_rs, dv_ss, dv_rs, s2_ss, s2_rs, zr_ss, zr_rs, za_ss, za_rs,
):
    z = lax.axis_index("sp")
    d = lax.axis_index("dp")
    c = lax.rem(d, 2)
    chip = lax.div(d, 2)
    xx = lax.rem(chip, nq)
    yy = lax.div(chip, nq)
    pa = xx * (1 - c) + yy * c
    pb = yy * (1 - c) + xx * c

    def chip_at(a, b):
        return (b * nq + a) * (1 - c) + (a * nq + b) * c

    def there(chip_id, core, at_z=None):
        return {"sp": z if at_z is None else at_z, "dp": chip_id * 2 + core}

    def turned(at, i, n):
        return lax.rem(at + i, n)

    barrier = pltpu.get_barrier_semaphore()
    greeted = 0
    for i in range(1, nq):
        for core in range(2):
            for other in (yy * nq + turned(xx, i, nq), turned(yy, i, nq) * nq + xx):
                pl.semaphore_signal(barrier, inc=1, device_id=there(other, core), device_id_type=MESH)
                greeted += 1
    pl.semaphore_signal(barrier, inc=1, device_id=there(chip, 1 - c), device_id_type=MESH)
    mate = z + 1 - 2 * lax.rem(z, 2)
    for at_z, core in (
        (mate, 0), (mate, 1), (turned(z, 2, nz), c), (turned(z, nz - 2, nz), c)
    ):
        pl.semaphore_signal(
            barrier, inc=1, device_id=there(chip, core, at_z), device_id_type=MESH
        )

    def left(ref, sem):
        remote(ref, ref, sem, sem, there(chip, 1 - c)).wait_send()

    def arrived(ref, sem):
        remote(ref, ref, sem, sem, there(chip, 1 - c)).wait_recv()

    named = ((g_in, g_ref), (q_in, q_ref), (k_in, k_ref), (v_in, v_ref), (cot_in, cot_ref))
    for h in range(2):
        for n, (a, b) in enumerate(named):
            for columns in (pl.ds(h * 256, 256), pl.ds(HALF + h * 256, 256)):
                pltpu.make_async_copy(a.at[:, columns], b.at[:, columns], in_sem.at[h, n]).start()

    def remote(src, dst, ss, rs, device):
        return pltpu.make_async_remote_copy(
            src_ref=src, dst_ref=dst, send_sem=ss, recv_sem=rs, device_id=device, device_id_type=MESH
        )

    row = lax.broadcasted_iota(jnp.int32, (BLOCK, BLOCK), 0)
    col = lax.broadcasted_iota(jnp.int32, (BLOCK, BLOCK), 1)
    left_half = lax.broadcasted_iota(jnp.int32, (64, 128), 1) < 64
    lane = lax.broadcasted_iota(jnp.int32, (BLOCK, 128), 1)
    mask0 = jnp.where(lane < 64, 1.0, 0.0).astype(BF16)
    mask1 = jnp.where(lane < 64, 0.0, 1.0).astype(BF16)
    upto = jnp.where(row >= col, 1.0, 0.0).astype(BF16)
    onward = jnp.where(row <= col, 1.0, 0.0).astype(BF16)

    def diagonal(m):
        return jnp.where(left_half, m[:64], m[64:])

    def pair_at(k):
        return lax.div(k, 2) + (PAIRS // 2) * lax.rem(k, 2)

    def place_of(p):
        return 4 * lax.rem(p, PAIRS // 2) + 2 * lax.div(p, PAIRS // 2)

    def local_states(k, _):
        p = pair_at(k)
        at = lanes(p * 128, 128)
        gate = g_ref[:, at]
        running = nn(upto, gate)
        exclusive = running - gate.astype(F32)
        run_s[:, at] = running
        end = jnp.exp(running[BLOCK - 1 : BLOCK])
        end_s[1, :, at] = jnp.broadcast_to(end, (8, 128))
        query = q_ref[:, at].astype(F32) * HEAD_DIM ** (-0.5)
        key = k_ref[:, at].astype(F32)
        qf = (query * jnp.exp(running)).astype(BF16)
        kf = (key * jnp.exp(-running)).astype(BF16)
        qb = (query * jnp.exp(-exclusive)).astype(BF16)
        kb = (key * jnp.exp(exclusive)).astype(BF16)
        qf_s[:, at] = qf
        kf_s[:, at] = kf
        qb_s[:, at] = qb
        kb_s[:, at] = kb
        value = v_ref[:, at]
        cot = cot_ref[:, at]
        uh = diagonal(tn(value, kf))
        wb = diagonal(tn(cot, qb))
        raw_s[2 * p] = uh
        raw_s[2 * p + 1] = wb
        place = 2 * k
        loc_s[1, 0, place] = (uh * end).astype(BF16)
        loc_s[1, 0, place + 1] = (wb * end).astype(BF16)
        loc_s[1, 1, place] = diagonal(tn(cot, qf)).astype(BF16)
        loc_s[1, 1, place + 1] = diagonal(tn(value, kb)).astype(BF16)
        return 0

    lead = 1 - lax.rem(z, 2)
    follow = 1 - lead
    quarter = CHUNKS // PARTS
    group = CHUNKS // 2

    def end_columns(h):
        return (pl.ds(h * 256, 256), pl.ds(HALF + h * 256, 256))

    for h in range(2):
        for n, (a, b) in enumerate(named):
            pltpu.make_async_copy(a.at[:, pl.ds(0, HALF)], b.at[:, pl.ds(0, HALF)], in_sem.at[h, n]).wait()
        lax.fori_loop(h * (PAIRS // 2), (h + 1) * (PAIRS // 2), local_states, 0, unroll=UNROLL)
        if h == 0:
            pl.semaphore_wait(barrier, greeted + 5)
        for columns in end_columns(h):
            remote(
                end_s.at[1, :, columns], fend_s.at[c, :, columns], fend_ss, fend_rs.at[c, h],
                there(chip, 1, mate),
            ).start()
        for n in range(h * PARTS // 2, (h + 1) * PARTS // 2):
            part = pl.ds(n * quarter, quarter)
            remote(
                loc_s.at[1, follow, part], fol_s.at[c, part], fol_ss, fol_rs.at[c, n],
                there(chip, 1, mate),
            ).start()

        @pl.when(c == 0)
        def _():
            for columns in end_columns(h):
                remote(
                    end_s.at[1, :, columns], end_s.at[0, :, columns],
                    loc_ss.at[1], loc_rs.at[1, h], there(chip, 1),
                ).start()
            part = pl.ds(h * group, group)
            remote(
                loc_s.at[1, lead, part], loc_s.at[0, lead, part],
                loc_ss.at[0], loc_rs.at[0, h], there(chip, 1),
            ).start()

    for half in range(2):
        columns = pl.ds(half * HALF, HALF)
        mine = wv_s.at[half, chip, pl.ds(pl.multiple_of(c * 64, 64), 64), :]

        @pl.when(c == 0)
        def _():
            pltpu.make_async_copy(w_ref.at[:, columns], mine, w_loc).start()

        @pl.when(c == 1)
        def _():
            remote(w_ref.at[:, columns], mine, w0_ss, w0_rs, there(chip, 0)).start()

    w_shard = wv_s.at[:, chip, pl.ds(0, 64), :]

    x_slot = (xx * 2 + c, yy * 2 + c)

    def x_copies(role, i):
        if role == 0:
            to = turned(xx, i, nq)
            target = there(yy * nq + to, 0)
            pieces = [
                (
                    x_ref.at[:, lanes((b * nq + to) * 128, 128)],
                    xg_s.at[x_slot[0], :, pl.ds(b * 128, 128)],
                )
                for b in range(nq)
            ]
        else:
            to = turned(yy, i, nq)
            target = there(to * nq + xx, 1)
            pieces = [(x_ref.at[:, lanes(to * nq * 128, nq * 128)], xg_s.at[x_slot[1]])]
        return target, pieces

    def send_x(role, i):
        target, pieces = x_copies(role, i)

        def away():
            for src, dst in pieces:
                remote(src, dst, x_ss, x_rs, target).start()

        def at_home():
            for src, dst in pieces:
                pltpu.make_async_copy(src, dst, x_rs).start()

        if i == 0:
            pl.when(c != role)(away)
            pl.when(c == role)(at_home)
        else:
            away()

    for role in range(2):
        for i in range(nq):
            send_x(role, i)

    def chip_in(half, a, b):
        return b * nq + a if half == 0 else a * nq + b

    w_at = ((xx, yy), (yy, xx))

    def w_first():
        pltpu.make_async_copy(w_shard, w_shard, w_loc).wait()
        arrived(w_shard, w0_rs)
        for half, (a, b) in enumerate(w_at):
            for i in range(1, nq):
                remote(
                    wv_s.at[half, chip], wv_s.at[half, chip], w1_ss, w1_rs.at[half],
                    there(chip_in(half, turned(a, i, nq), b), 0),
                ).start()

    def both(a):
        return jnp.concatenate([a * mask0, a * mask1], axis=0)

    row2 = lax.broadcasted_iota(jnp.int32, (BLOCK, 256), 0)
    col2 = lax.rem(lax.broadcasted_iota(jnp.int32, (BLOCK, 256), 1), 128)
    lower = row2 >= col2
    upper = row2 <= col2

    def own_part(p, _):
        at = lanes(p * 128, 128)
        value = v_ref[:, at]
        cot = cot_ref[:, at]
        qf, kf, qb, kb = qf_s[:, at], kf_s[:, at], qb_s[:, at], kb_s[:, at]
        value2, cot2 = both(value), both(cot)
        qf2, kf2, qb2, kb2 = both(qf), both(kf), both(qb), both(kb)
        d_score = nt(cot, value2)
        d_score_t = nt(value, cot2)
        score_t = jnp.where(upper, nt(kf, qf2), 0.0) + jnp.where(lower, nt(kb, qb2), 0.0)
        dqf_s[:, at] = nn(jnp.where(lower, d_score, 0.0).astype(BF16), kf2)
        dqb_s[:, at] = nn(jnp.where(upper, d_score, 0.0).astype(BF16), kb2)
        dkf_s[:, at] = nn(jnp.where(upper, d_score_t, 0.0).astype(BF16), qf2)
        dkb_s[:, at] = nn(jnp.where(lower, d_score_t, 0.0).astype(BF16), qb2)
        dv_s[:, at] = nn(score_t.astype(BF16), cot2)
        return 0

    def own_parts():
        lax.fori_loop(0, PAIRS, own_part, 0, unroll=UNROLL)

    def turn_inputs():
        arrived(xg_s, x_rs)
        for slot in range(2 * nq):
            for b in range(nq):
                xgt_s[b * 128 : (b + 1) * 128, slot * BLOCK : (slot + 1) * BLOCK] = xg_s[
                    slot, :, b * 128 : (b + 1) * 128
                ].T

    def w_second():
        for half, (a, b) in enumerate(w_at):
            arrived(wv_s.at[0, pl.ds(0, nq - 1)], w1_rs.at[half])
            for i in range(1, nq):
                for j in range(nq):
                    block = wv_s.at[half, chip_in(half, j, b)]
                    remote(
                        block, block, w2_ss, w2_rs,
                        there(chip_in(half, a, turned(b, i, nq)), 0),
                    ).start()

    def before(way):
        return z + way * (nz - 1 - 2 * z)

    for way in range(2):

        @pl.when(before(way) == 0)
        def _():
            state_s[:, way] = jnp.zeros((2, *state_s.shape[2:]), BF16)

    @pl.when(before(lead) == 1)
    def _():
        in_s[...] = jnp.zeros(in_s.shape, BF16)

    def onward_copy(s, i):
        return remote(
            out_s.at[s, i], in_s.at[s, i], chain_ss.at[s], chain_rs.at[s, i],
            there(chip, 1, lax.rem(z + 2 - 4 * lead + nz, nz)),
        )

    def hand_copy(s, i, way):
        return remote(
            in_s.at[s, i], state_s.at[s, way, i], hand_ss.at[s], hand_rs.at[s, i],
            there(chip, 1, mate),
        )

    def forward_copy(way, i):
        return remote(
            state_s.at[0, way, i], state_s.at[1, way, i],
            fw_ss.at[way], fw_rs.at[lax.div(i, quarter), way], there(chip, 1 - c),
        )

    edge = jnp.minimum(z, nz - 1 - z)
    first = jnp.where(edge >= nz // 4, lead, lax.div(2 * z, nz))
    steps = 2 * CHUNKS

    def taken(index):
        part = lax.div(index, 2 * quarter)
        rest = lax.rem(index, 2 * quarter)
        s = 1 - lax.rem(part + lax.div(rest, quarter), 2)
        return s, part * quarter + lax.rem(rest, quarter)

    def lead_step(index, _):
        s, i = taken(index)
        onward = onward_copy(s, i)

        @pl.when(lax.rem(i, group) == 0)
        def _():
            half = lax.div(i, group)
            arrived(fend_s.at[0, :, pl.ds(0, HALF)], fend_rs.at[s, half])

            @pl.when(s == 0)
            def _():
                arrived(end_s.at[0, :, pl.ds(0, HALF)], loc_rs.at[1, half])
                arrived(loc_s.at[0, lead, pl.ds(0, group)], loc_rs.at[0, half])

        @pl.when(lax.rem(i, quarter) == 0)
        def _():
            arrived(fol_s.at[0, pl.ds(0, quarter)], fol_rs.at[s, lax.div(i, quarter)])

        @pl.when(before(lead) > 1)
        def _():
            onward.wait_recv()

        at = lanes(pair_at(lax.div(i, 2)) * 128, 128)
        state = in_s[s, i].astype(F32) * fend_s[s, 0:1, at] + fol_s[s, i].astype(F32)
        state_s[s, lead, i] = state.astype(BF16)

        @pl.when(before(lead) < nz - 1)
        def _():
            behind = state * end_s[s, 0:1, at] + loc_s[s, lead, i].astype(F32)
            out_s[s, i] = behind.astype(BF16)
            onward.start()

        @pl.when(before(lead) > 1)
        def _():
            hand_copy(s, i, lead).start()

        @pl.when(s == 0)
        def _():
            forward_copy(lead, i).start()

        return 0

    def follow_step(index, _):
        s, i = taken(index)
        hand_copy(s, i, follow).wait_recv()

        @pl.when(s == 0)
        def _():
            forward_copy(follow, i).start()

        return 0

    def chain(way, begin, end):
        @pl.when((c == 1) & (way == lead))
        def _():
            lax.fori_loop(begin, end, lead_step, 0)

        @pl.when((c == 1) & (way != lead) & (before(follow) > 0))
        def _():
            lax.fori_loop(begin, end, follow_step, 0)

    pl.when(c == 0)(w_first)
    pl.when((c == 0) | (edge >= nz // 4))(own_parts)
    chain(first, 0, steps)
    pl.when((c == 1) & (edge < nz // 4))(own_parts)
    pl.when(c == 0)(w_second)
    pl.when((c == 0) | (edge < 2))(turn_inputs)

    def spread(state):
        zero = jnp.zeros_like(state)
        return jnp.concatenate(
            [jnp.where(left_half, state, zero), jnp.where(left_half, zero, state)], axis=0
        ).astype(BF16)

    def value_part(i, _):
        p = pair_at(i)
        at = lanes(p * 128, 128)
        e2 = spread(state_s[1, 1, 2 * i].astype(F32) * end_s[1, 0:1, at])
        f2 = spread(state_s[1, 0, 2 * i + 1].astype(F32))
        dvb_s[:, at] = (dv_s[:, at] + nt(kf_s[:, at], e2) + nt(kb_s[:, at], f2)).astype(BF16)
        return 0

    def w_swap():
        arrived(wv_s.at[:, pl.ds(0, (nq - 1) * nq)], w2_rs)
        remote(wv_s, wv_s, w3_ss, w3_rs, there(chip, 1)).start()

    def send_dv(h, role, i):
        if role == 0:
            target = there(yy * nq + turned(xx, i, nq), 0)
        else:
            target = there(turned(yy, i, nq) * nq + xx, 1)
        src = dvb_s.at[:, pl.ds(role * HALF + h * 128, 128)]
        dst = dvg_s.at[h, x_slot[role]]

        def away():
            remote(src, dst, dv_ss, dv_rs.at[h], target).start()

        def at_home():
            pltpu.make_async_copy(src, dst, dv_rs.at[h]).start()

        if i == 0:
            pl.when(c != role)(away)
            pl.when(c == role)(at_home)
        else:
            away()

    def back(h):
        for way in range(2):

            @pl.when((c == 0) & (before(way) > 0))
            def _():
                arrived(state_s.at[1, way, pl.ds(0, quarter)], fw_rs.at[h, way])

    for h in range(PARTS):
        chain(1 - first, 2 * h * quarter, 2 * (h + 1) * quarter)
        back(h)
        lax.fori_loop(2 * h, 2 * h + 2, value_part, 0, unroll=2)
        for i in (2, 1, 3, 0) if nq == 4 else (1, 0):
            for role in range(2):
                send_dv(h, role, i)

    def finish(p, _):
        at = lanes(p * 128, 128)
        value = v_ref[:, at]
        cot = cot_ref[:, at]
        qf, kf, qb, kb = qf_s[:, at], kf_s[:, at], qb_s[:, at], kb_s[:, at]
        end = end_s[1, 0:1, at]
        place = place_of(p)
        h_state = state_s[1, 0, place].astype(F32)
        f_state = state_s[1, 0, place + 1].astype(F32)
        e_state = (state_s[1, 1, place].astype(F32) * end).astype(BF16).astype(F32)
        r_state = (state_s[1, 1, place + 1].astype(F32) * end).astype(BF16).astype(F32)
        carry = jnp.sum(
            e_state * (h_state + raw_s[2 * p]) + r_state * (f_state + raw_s[2 * p + 1]),
            axis=0,
            keepdims=True,
        )
        h2, f2, e2, r2 = spread(h_state), spread(f_state), spread(e_state), spread(r_state)
        dqf = dqf_s[:, at] + nn(cot, h2)
        dqb = dqb_s[:, at] + nn(cot, r2)
        dkf = dkf_s[:, at] + nn(value, e2)
        dkb = dkb_s[:, at] + nn(value, f2)
        running = run_s[:, at]
        exclusive = running - g_ref[:, at].astype(F32)
        dq = (jnp.exp(running) * dqf + jnp.exp(-exclusive) * dqb) * HEAD_DIM ** (-0.5)
        dk = jnp.exp(-running) * dkf + jnp.exp(exclusive) * dkb
        dq_ref[:, at] = dq.astype(BF16)
        dk_ref[:, at] = dk.astype(BF16)
        fwd = qf.astype(F32) * dqf - kf.astype(F32) * dkf
        bwd = kb.astype(F32) * dkb - qb.astype(F32) * dqb
        both_ways = fwd + bwd
        high = both_ways.astype(BF16)
        low = (both_ways - high.astype(F32)).astype(BF16)
        dg = nn(onward, high) + nn(onward, low) - bwd + carry
        dg_ref[:, at] = dg.astype(BF16)
        return 0

    pl.when((c == 1) & (edge >= 2))(turn_inputs)
    pl.when(c == 0)(w_swap)
    lax.fori_loop(0, PAIRS, finish, 0, unroll=UNROLL)

    outputs = [
        pltpu.make_async_copy(a, b, out_sem.at[n])
        for n, (a, b) in enumerate(
            ((dq_ref, dq_out), (dk_ref, dk_out), (dg_ref, dg_out), (gi_ref, gi_out))
        )
    ]
    for copy in outputs[:3]:
        copy.start()

    tokens = 2 * nq * BLOCK

    def s2_copies(h):
        return [
            remote(
                pb_s.at[h, turned(pb, i, nq)], s2_s.at[h, i - 1],
                s2_ss.at[h], s2_rs.at[h],
                there(chip_at(pa, turned(pb, i, nq)), c),
            )
            for i in range(1, nq)
        ]

    for h in range(PARTS):
        arrived(dvg_s.at[h], dv_rs.at[h])
        part = nn(xgt_s[...], dvg_s[h].reshape(tokens, 128))
        part_s[h] = part.reshape(nq, 128, 128)
        pb_s[h] = part.astype(BF16).reshape(nq, 128, 128)
        for copy in s2_copies(h):
            copy.start()

    wide = PARTS
    stack = nz // wide
    height = 128 // stack

    per = stack // 2

    def summing(r, part):
        if r < per:
            return nz // 2 + part * per + r
        return (PARTS - 1 - part) * per + r - per

    def z_copy(to):
        return remote(zb_s.at[to], zr_s.at[z], zr_ss, zr_rs, there(chip, c, to))

    for h in range(PARTS):
        total = part_s[h, pb]
        arrived(s2_s.at[h], s2_rs.at[h])
        for i in range(nq - 1):
            total = total + s2_s[h, i].astype(F32)
        for r in range(stack):
            zb_s[summing(r, h)] = total[r * height : (r + 1) * height].astype(BF16)
        for r in range(stack):
            to = summing(r, h)
            pl.when(to != z)(lambda: z_copy(to).start())

    zr_s[z] = zb_s[z]

    arrived(zr_s.at[pl.ds(0, nz - 1)], zr_rs)
    rb_s[...] = jnp.sum(zr_s[...].astype(F32), axis=0).astype(BF16)

    upper_z = lax.div(2 * z, nz)
    owner = 1 - upper_z
    depth = lax.div(lax.rem(z, nz // 2), per)
    part_here = depth * upper_z + (PARTS - 1 - depth) * (1 - upper_z)
    slot = c * (nz // 2) + part_here * per + lax.rem(z, per)

    def out_copy(i):
        return remote(
            rb_s, gr_s.at[slot], za_ss, za_rs, there(chip, owner, turned(z, i, nz))
        )

    home = pltpu.make_async_copy(rb_s, gr_s.at[slot], za_rs)
    for near in range(nz // 2):
        out_copy(nz // 2 - near).start()
        if near > 0:
            out_copy(nz // 2 + near).start()
    pl.when(owner == c)(lambda: home.start())
    pl.when(owner != c)(lambda: out_copy(0).start())

    pl.when(c == 1)(lambda: arrived(wv_s, w3_rs))
    group = nq * 128
    for i in range(nq):
        low_half = wv_s[0, i * nq : (i + 1) * nq].reshape(group, HALF)
        high_half = wv_s[1, i * nq : (i + 1) * nq].reshape(group, HALF)
        gi_ref[:, i * group : (i + 1) * group] = (
            nt(dvb_s[:, :HALF], low_half) + nt(dvb_s[:, HALF:], high_half)
        ).astype(BF16)

    outputs[3].start()

    arrived(gr_s, za_rs)

    for copy in outputs:
        copy.wait()
    left(zr_s.at[pl.ds(0, nz - 1)], zr_ss)
    for h in range(PARTS):
        left(s2_s.at[h], s2_ss.at[h])
    pl.when(owner == c)(lambda: left(zr_s.at[pl.ds(0, nz - 1)], za_ss))
    pl.when(owner != c)(lambda: left(zr_s, za_ss))

    @pl.when(c == 0)
    def _():
        left(loc_s.at[1, lead], loc_ss.at[0])
        left(end_s.at[1], loc_ss.at[1])

    left(end_s.at[1], fend_ss)
    left(fol_s.at[0], fol_ss)

    @pl.when((c == 1) & (before(lead) < nz - 1))
    def _():
        for s in range(2):
            left(out_s.at[s], chain_ss.at[s])

    @pl.when((c == 1) & (before(lead) > 1))
    def _():
        for s in range(2):
            left(in_s.at[s], hand_ss.at[s])

    for way in range(2):

        @pl.when((c == 1) & (before(way) > 0))
        def _():
            left(state_s.at[0, way], fw_ss.at[way])

    @pl.when(c == 0)
    def _():
        left(wv_s.at[:, pl.ds(0, nq - 1)], w1_ss)
        left(wv_s.at[:, pl.ds(0, (nq - 1) * nq)], w2_ss)
        left(wv_s, w3_ss)

    @pl.when(c == 1)
    def _():
        left(w_shard, w0_ss)

    left(xg_s.at[pl.ds(0, 2 * nq - 1)], x_ss)
    left(dvg_s.at[:, pl.ds(0, 2 * nq - 1)], dv_ss)


def store(dq, dk, dg, gi, gr, dq_out, dk_out, dg_out, gi_out, gw_out, gw_s, sems):
    copies = [
        pltpu.make_async_copy(a, b, sems.at[n])
        for n, (a, b) in enumerate(((gi, gi_out), (dq, dq_out), (dk, dk_out), (dg, dg_out)))
    ]
    for copy in copies:
        copy.start()
    count, height, chunk = gr.shape
    for s in range(count):
        role, t = s // (count // 2), s % (count // 2)
        per = count // 2 // PARTS
        rows, columns = t % per * height, role * HALF + t // per * chunk
        gw_s[rows : rows + height, columns : columns + chunk] = gr[s].astype(F32)
    last = pltpu.make_async_copy(gw_s, gw_out, sems.at[4])
    last.start()
    for copy in (*copies, last):
        copy.wait()


def per_device(nz, nq, inputs, queries, keys, values, log_decay, cotangent, value_weight):
    model = inputs.shape[2]
    slots = 2 * nq
    wide = PARTS
    chunk = (128 * wide // nz, HALF // wide)
    dma = pltpu.SemaphoreType.DMA
    vm = pltpu.VMEM
    shapes = [((BLOCK, WIDTH), BF16)] * 3 + [((BLOCK, model), BF16)]
    sums = ((nz, *chunk), BF16)
    weight = ((64, WIDTH), F32)
    in_vmem = pl.BlockSpec(memory_space=pltpu.VMEM)
    anywhere = pl.BlockSpec(memory_space=pl.ANY)
    outs = pl.pallas_call(
        functools.partial(kernel, nz, nq),
        out_shape=tuple(vm(*shape) for shape in (*shapes, sums)),
        in_specs=[anywhere] * 7,
        out_specs=[anywhere] * 5,
        scratch_shapes=[
            *[vm((BLOCK, WIDTH), BF16)] * 8,
            vm((BLOCK, model), BF16),
            vm((BLOCK, WIDTH), F32),
            vm((2, 8, WIDTH), F32),
            *[vm((BLOCK, WIDTH), BF16)] * 4,
            vm((2, 2, CHUNKS, 64, 128), BF16),
            vm((CHUNKS, 64, 128), F32),
            vm((2, CHUNKS, 64, 128), BF16),
            vm((2, 8, WIDTH), F32),
            vm((2, CHUNKS, 64, 128), BF16),
            vm((2, CHUNKS, 64, 128), BF16),
            vm((2, 2, CHUNKS, 64, 128), BF16),
            *[vm((BLOCK, WIDTH), F32)] * 5,
            vm((BLOCK, WIDTH), BF16),
            vm((2, nq * nq, 128, HALF), BF16),
            vm((slots, BLOCK, nq * 128), BF16),
            vm((nq * 128, slots * BLOCK), BF16),
            vm((PARTS, slots, BLOCK, 128), BF16),
            vm((PARTS, nq, 128, 128), F32),
            vm((PARTS, nq, 128, 128), BF16),
            vm((PARTS, nq - 1, 128, 128), BF16),
            vm(*sums),
            vm(*sums),
            vm(chunk, BF16),
            dma((2, 5)), dma((4,)),
            dma((2,)), dma((2, CHUNKS)),
            dma((2,)), dma((2, CHUNKS)),
            dma((2,)), dma((PARTS, 2)),
            dma((2,)), dma((2, 2)),
            dma, dma((2, PARTS)),
            dma, dma((2, 2)),
            *[dma] * 4,
            dma((2,)),
            *[dma] * 7,
            dma((PARTS,)),
            dma((PARTS,)), dma((PARTS,)),
            *[dma] * 4,
        ],
        compiler_params=pltpu.CompilerParams(
            collective_id=0, has_side_effects=True, vmem_limit_bytes=65_300_000
        ),
    )(
        queries[0], keys[0], values[0], log_decay[0], cotangent[0], inputs[0], value_weight
    )
    dq, dk, dg, gi, gw = pl.pallas_call(
        store,
        out_shape=tuple(jax.ShapeDtypeStruct(*shape) for shape in (*shapes, weight)),
        in_specs=[anywhere] * 4 + [in_vmem],
        out_specs=[anywhere] * 5,
        scratch_shapes=[vm(*weight), dma((5,))],
        compiler_params=pltpu.CompilerParams(vmem_limit_bytes=1024 * 1024),
    )(*outs)
    return dq[None], dk[None], dg[None], gi[None], gw


def solution(mesh):
    nz = mesh.shape["sp"]
    nq = 4 if mesh.shape["dp"] == 32 else 2
    tokens = P("dp", "sp", None)
    return jax.shard_map(
        functools.partial(per_device, nz, nq),
        mesh=mesh,
        in_specs=(tokens,) * 6 + (P("dp", None),),
        out_specs=(tokens,) * 4 + (P("dp", None),),
        check_vma=False,
    )
```

```python
import functools

import jax
import jax.numpy as jnp
from jax import lax
from jax.experimental import pallas as pl
from jax.experimental.pallas import tpu as pltpu
from jax.sharding import PartitionSpec as P

MESH = pl.DeviceIdType.MESH
F32 = jnp.float32
BF16 = jnp.bfloat16
BLOCK = 128
WIDTH = 1024
HALF = WIDTH // 2
PAIRS = WIDTH // 128
CHUNKS = 2 * PAIRS
HEAD_DIM = 64
UNROLL = 4
PARTS = 4


def nn(a, b):
    return lax.dot_general(a, b, (((1,), (0,)), ((), ())), preferred_element_type=F32)


def nt(a, b):
    return lax.dot_general(a, b, (((1,), (1,)), ((), ())), preferred_element_type=F32)


def tn(a, b):
    return lax.dot_general(a, b, (((0,), (0,)), ((), ())), preferred_element_type=F32)


def lanes(start, size):
    return pl.ds(pl.multiple_of(start, 128), size)


def kernel(
    nz, nq,
    q_in, k_in, v_in, g_in, cot_in, x_ref, w_ref,
    dq_out, dk_out, dg_out, gi_out, gr_s,
    q_ref, k_ref, v_ref, g_ref, cot_ref, dq_ref, dk_ref, dg_ref, gi_ref,
    run_s, end_s, qf_s, kf_s, qb_s, kb_s, loc_s, raw_s,
    fol_s, fend_s, in_s, out_s, state_s,
    dqf_s, dqb_s, dkf_s, dkb_s, dv_s, dvb_s,
    wv_s, xg_s, xgt_s, dvg_s, part_s, pb_s, s2_s, zb_s, zr_s, rb_s,
    in_sem, out_sem, chain_ss, chain_rs, hand_ss, hand_rs, fw_ss, fw_rs,
    loc_ss, loc_rs, fol_ss, fol_rs, fend_ss, fend_rs,
    w0_ss, w0_rs, w_loc, w1_ss, w1_rs, w2_ss, w2_rs, w3_ss, w3_rs,
    x_ss, x_rs, dv_ss, dv_rs, s2_ss, s2_rs, zr_ss, zr_rs, za_ss, za_rs,
):
    z = lax.axis_index("sp")
    d = lax.axis_index("dp")
    c = lax.rem(d, 2)
    chip = lax.div(d, 2)
    xx = lax.rem(chip, nq)
    yy = lax.div(chip, nq)
    pa = xx * (1 - c) + yy * c
    pb = yy * (1 - c) + xx * c

    def chip_at(a, b):
        return (b * nq + a) * (1 - c) + (a * nq + b) * c

    def there(chip_id, core, at_z=None):
        return {"sp": z if at_z is None else at_z, "dp": chip_id * 2 + core}

    def turned(at, i, n):
        return lax.rem(at + i, n)

    barrier = pltpu.get_barrier_semaphore()
    greeted = 0
    for i in range(1, nq):
        for core in range(2):
            for other in (yy * nq + turned(xx, i, nq), turned(yy, i, nq) * nq + xx):
                pl.semaphore_signal(barrier, inc=1, device_id=there(other, core), device_id_type=MESH)
                greeted += 1
    pl.semaphore_signal(barrier, inc=1, device_id=there(chip, 1 - c), device_id_type=MESH)
    mate = z + 1 - 2 * lax.rem(z, 2)
    for at_z, core in (
        (mate, 0), (mate, 1), (turned(z, 2, nz), c), (turned(z, nz - 2, nz), c)
    ):
        pl.semaphore_signal(
            barrier, inc=1, device_id=there(chip, core, at_z), device_id_type=MESH
        )

    def left(ref, sem):
        remote(ref, ref, sem, sem, there(chip, 1 - c)).wait_send()

    def arrived(ref, sem):
        remote(ref, ref, sem, sem, there(chip, 1 - c)).wait_recv()

    named = ((g_in, g_ref), (q_in, q_ref), (k_in, k_ref), (v_in, v_ref), (cot_in, cot_ref))
    for h in range(2):
        for a, b in named:
            for columns in (pl.ds(h * 256, 256), pl.ds(HALF + h * 256, 256)):
                pltpu.make_async_copy(a.at[:, columns], b.at[:, columns], in_sem.at[h]).start()

    def remote(src, dst, ss, rs, device):
        return pltpu.make_async_remote_copy(
            src_ref=src, dst_ref=dst, send_sem=ss, recv_sem=rs, device_id=device, device_id_type=MESH
        )

    row = lax.broadcasted_iota(jnp.int32, (BLOCK, BLOCK), 0)
    col = lax.broadcasted_iota(jnp.int32, (BLOCK, BLOCK), 1)
    left_half = lax.broadcasted_iota(jnp.int32, (64, 128), 1) < 64
    lane = lax.broadcasted_iota(jnp.int32, (BLOCK, 128), 1)
    mask0 = jnp.where(lane < 64, 1.0, 0.0).astype(BF16)
    mask1 = jnp.where(lane < 64, 0.0, 1.0).astype(BF16)
    upto = jnp.where(row >= col, 1.0, 0.0).astype(BF16)
    onward = jnp.where(row <= col, 1.0, 0.0).astype(BF16)

    def diagonal(m):
        return jnp.where(left_half, m[:64], m[64:])

    def pair_at(k):
        return lax.div(k, 2) + (PAIRS // 2) * lax.rem(k, 2)

    def place_of(p):
        return 4 * lax.rem(p, PAIRS // 2) + 2 * lax.div(p, PAIRS // 2)

    def local_states(k, _):
        p = pair_at(k)
        at = lanes(p * 128, 128)
        gate = g_ref[:, at]
        running = nn(upto, gate)
        exclusive = running - gate.astype(F32)
        run_s[:, at] = running
        end = jnp.exp(running[BLOCK - 1 : BLOCK])
        end_s[1, :, at] = jnp.broadcast_to(end, (8, 128))
        query = q_ref[:, at].astype(F32) * HEAD_DIM ** (-0.5)
        key = k_ref[:, at].astype(F32)
        qf = (query * jnp.exp(running)).astype(BF16)
        kf = (key * jnp.exp(-running)).astype(BF16)
        qb = (query * jnp.exp(-exclusive)).astype(BF16)
        kb = (key * jnp.exp(exclusive)).astype(BF16)
        qf_s[:, at] = qf
        kf_s[:, at] = kf
        qb_s[:, at] = qb
        kb_s[:, at] = kb
        value = v_ref[:, at]
        cot = cot_ref[:, at]
        uh = diagonal(tn(value, kf))
        wb = diagonal(tn(cot, qb))
        raw_s[2 * p] = uh
        raw_s[2 * p + 1] = wb
        place = 2 * k
        loc_s[1, 0, place] = (uh * end).astype(BF16)
        loc_s[1, 0, place + 1] = (wb * end).astype(BF16)
        loc_s[1, 1, place] = diagonal(tn(cot, qf)).astype(BF16)
        loc_s[1, 1, place + 1] = diagonal(tn(value, kb)).astype(BF16)
        return 0

    lead = 1 - lax.rem(z, 2)
    follow = 1 - lead
    quarter = CHUNKS // PARTS
    group = CHUNKS // 2

    def half_inputs():
        return wv_s.at[0, pl.ds(0, 5)] if nq == 4 else xg_s.at[:, :, pl.ds(0, 128)]

    def end_columns(h):
        return (pl.ds(h * 256, 256), pl.ds(HALF + h * 256, 256))

    for h in range(2):
        taken_in = half_inputs()
        pltpu.make_async_copy(taken_in, taken_in, in_sem.at[h]).wait()
        lax.fori_loop(h * (PAIRS // 2), (h + 1) * (PAIRS // 2), local_states, 0, unroll=UNROLL)
        if h == 0:
            pl.semaphore_wait(barrier, greeted + 5)
        for columns in end_columns(h):
            remote(
                end_s.at[1, :, columns], fend_s.at[c, :, columns], fend_ss, fend_rs.at[c, h],
                there(chip, 1, mate),
            ).start()
        for n in range(h * PARTS // 2, (h + 1) * PARTS // 2):
            part = pl.ds(n * quarter, quarter)
            remote(
                loc_s.at[1, follow, part], fol_s.at[c, part], fol_ss, fol_rs.at[c, n],
                there(chip, 1, mate),
            ).start()

        @pl.when(c == 0)
        def _():
            for columns in end_columns(h):
                remote(
                    end_s.at[1, :, columns], end_s.at[0, :, columns],
                    loc_ss.at[1], loc_rs.at[1, h], there(chip, 1),
                ).start()
            part = pl.ds(h * group, group)
            remote(
                loc_s.at[1, lead, part], loc_s.at[0, lead, part],
                loc_ss.at[0], loc_rs.at[0, h], there(chip, 1),
            ).start()

    for half in range(2):
        columns = pl.ds(half * HALF, HALF)
        mine = wv_s.at[half, chip, pl.ds(pl.multiple_of(c * 64, 64), 64), :]

        @pl.when(c == 0)
        def _():
            pltpu.make_async_copy(w_ref.at[:, columns], mine, w_loc).start()

        @pl.when(c == 1)
        def _():
            remote(w_ref.at[:, columns], mine, w0_ss, w0_rs, there(chip, 0)).start()

    w_shard = wv_s.at[:, chip, pl.ds(0, 64), :]

    x_slot = (xx * 2 + c, yy * 2 + c)

    def x_copies(role, i):
        if role == 0:
            to = turned(xx, i, nq)
            target = there(yy * nq + to, 0)
            pieces = [
                (
                    x_ref.at[:, lanes((b * nq + to) * 128, 128)],
                    xg_s.at[x_slot[0], :, pl.ds(b * 128, 128)],
                )
                for b in range(nq)
            ]
        else:
            to = turned(yy, i, nq)
            target = there(to * nq + xx, 1)
            pieces = [(x_ref.at[:, lanes(to * nq * 128, nq * 128)], xg_s.at[x_slot[1]])]
        return target, pieces

    def send_x(role, i):
        target, pieces = x_copies(role, i)

        def away():
            for src, dst in pieces:
                remote(src, dst, x_ss, x_rs, target).start()

        def at_home():
            for src, dst in pieces:
                pltpu.make_async_copy(src, dst, x_rs).start()

        if i == 0:
            pl.when(c != role)(away)
            pl.when(c == role)(at_home)
        else:
            away()

    for role in range(2):
        for i in range(nq):
            send_x(role, i)

    def chip_in(half, a, b):
        return b * nq + a if half == 0 else a * nq + b

    w_at = ((xx, yy), (yy, xx))

    def w_first():
        pltpu.make_async_copy(w_shard, w_shard, w_loc).wait()
        arrived(w_shard, w0_rs)
        for half, (a, b) in enumerate(w_at):
            for i in range(1, nq):
                remote(
                    wv_s.at[half, chip], wv_s.at[half, chip], w1_ss, w1_rs.at[half],
                    there(chip_in(half, turned(a, i, nq), b), 0),
                ).start()

    def both(a):
        return jnp.concatenate([a * mask0, a * mask1], axis=0)

    row2 = lax.broadcasted_iota(jnp.int32, (BLOCK, 256), 0)
    col2 = lax.rem(lax.broadcasted_iota(jnp.int32, (BLOCK, 256), 1), 128)
    lower = row2 >= col2
    upper = row2 <= col2

    def own_part(p, _):
        at = lanes(p * 128, 128)
        value = v_ref[:, at]
        cot = cot_ref[:, at]
        qf, kf, qb, kb = qf_s[:, at], kf_s[:, at], qb_s[:, at], kb_s[:, at]
        value2, cot2 = both(value), both(cot)
        qf2, kf2, qb2, kb2 = both(qf), both(kf), both(qb), both(kb)
        d_score = nt(cot, value2)
        d_score_t = nt(value, cot2)
        score_t = jnp.where(upper, nt(kf, qf2), 0.0) + jnp.where(lower, nt(kb, qb2), 0.0)
        dqf_s[:, at] = nn(jnp.where(lower, d_score, 0.0).astype(BF16), kf2)
        dqb_s[:, at] = nn(jnp.where(upper, d_score, 0.0).astype(BF16), kb2)
        dkf_s[:, at] = nn(jnp.where(upper, d_score_t, 0.0).astype(BF16), qf2)
        dkb_s[:, at] = nn(jnp.where(lower, d_score_t, 0.0).astype(BF16), qb2)
        dv_s[:, at] = nn(score_t.astype(BF16), cot2)
        return 0

    def own_parts():
        lax.fori_loop(0, PAIRS, own_part, 0, unroll=UNROLL)

    def turn_inputs():
        arrived(xg_s, x_rs)
        for slot in range(2 * nq):
            for b in range(nq):
                xgt_s[b * 128 : (b + 1) * 128, slot * BLOCK : (slot + 1) * BLOCK] = xg_s[
                    slot, :, b * 128 : (b + 1) * 128
                ].T

    def w_second():
        for half, (a, b) in enumerate(w_at):
            arrived(wv_s.at[0, pl.ds(0, nq - 1)], w1_rs.at[half])
            for i in range(1, nq):
                for j in range(nq):
                    block = wv_s.at[half, chip_in(half, j, b)]
                    remote(
                        block, block, w2_ss, w2_rs,
                        there(chip_in(half, a, turned(b, i, nq)), 0),
                    ).start()

    def before(way):
        return z + way * (nz - 1 - 2 * z)

    for way in range(2):

        @pl.when(before(way) == 0)
        def _():
            state_s[:, way] = jnp.zeros((2, *state_s.shape[2:]), BF16)

    @pl.when(before(lead) == 1)
    def _():
        in_s[...] = jnp.zeros(in_s.shape, BF16)

    def onward_copy(s, i):
        return remote(
            out_s.at[s, i], in_s.at[s, i], chain_ss.at[s], chain_rs.at[s, i],
            there(chip, 1, lax.rem(z + 2 - 4 * lead + nz, nz)),
        )

    def hand_copy(s, i, way):
        return remote(
            in_s.at[s, i], state_s.at[s, way, i], hand_ss.at[s], hand_rs.at[s, lax.div(i, quarter)],
            there(chip, 1, mate),
        )

    def forward_copy(way, i, count=1):
        part = pl.ds(i, count)
        return remote(
            state_s.at[0, way, part], state_s.at[1, way, part],
            fw_ss.at[way], fw_rs.at[lax.div(i, quarter), way], there(chip, 1 - c),
        )

    edge = jnp.minimum(z, nz - 1 - z)
    first = jnp.where(edge >= nz // 4, lead, lax.div(2 * z, nz))
    steps = 2 * CHUNKS

    def taken(index):
        part = lax.div(index, 2 * quarter)
        rest = lax.rem(index, 2 * quarter)
        s = 1 - lax.rem(part + lax.div(rest, quarter), 2)
        return s, part * quarter + lax.rem(rest, quarter)

    def lead_step(index, _):
        s, i = taken(index)
        onward = onward_copy(s, i)

        @pl.when(lax.rem(i, group) == 0)
        def _():
            half = lax.div(i, group)
            arrived(fend_s.at[0, :, pl.ds(0, HALF)], fend_rs.at[s, half])

            @pl.when(s == 0)
            def _():
                arrived(end_s.at[0, :, pl.ds(0, HALF)], loc_rs.at[1, half])
                arrived(loc_s.at[0, lead, pl.ds(0, group)], loc_rs.at[0, half])

        @pl.when(lax.rem(i, quarter) == 0)
        def _():
            arrived(fol_s.at[0, pl.ds(0, quarter)], fol_rs.at[s, lax.div(i, quarter)])

        @pl.when(before(lead) > 1)
        def _():
            onward.wait_recv()

        at = lanes(pair_at(lax.div(i, 2)) * 128, 128)
        state = in_s[s, i].astype(F32) * fend_s[s, 0:1, at] + fol_s[s, i].astype(F32)
        state_s[s, lead, i] = state.astype(BF16)

        @pl.when(before(lead) < nz - 1)
        def _():
            behind = state * end_s[s, 0:1, at] + loc_s[s, lead, i].astype(F32)
            out_s[s, i] = behind.astype(BF16)
            onward.start()

        @pl.when(before(lead) > 1)
        def _():
            hand_copy(s, i, lead).start()

        @pl.when(s == 0)
        def _():
            forward_copy(lead, i).start()

        return 0

    def follow_step(index, _):
        s, i = taken(index * quarter)
        arrived(state_s.at[0, follow, pl.ds(0, quarter)], hand_rs.at[s, lax.div(i, quarter)])

        @pl.when(s == 0)
        def _():
            forward_copy(follow, i, quarter).start()

        return 0

    def chain(way, begin, end):
        @pl.when((c == 1) & (way == lead))
        def _():
            lax.fori_loop(begin, end, lead_step, 0)

        @pl.when((c == 1) & (way != lead) & (before(follow) > 0))
        def _():
            lax.fori_loop(begin // quarter, end // quarter, follow_step, 0)

    pl.when(c == 0)(w_first)
    pl.when((c == 0) | (edge >= nz // 4))(own_parts)
    chain(first, 0, steps)
    pl.when((c == 1) & (edge < nz // 4))(own_parts)
    pl.when(c == 0)(w_second)
    pl.when((c == 0) | (edge < 2))(turn_inputs)

    def spread(state):
        zero = jnp.zeros_like(state)
        return jnp.concatenate(
            [jnp.where(left_half, state, zero), jnp.where(left_half, zero, state)], axis=0
        ).astype(BF16)

    def value_part(i, _):
        p = pair_at(i)
        at = lanes(p * 128, 128)
        e2 = spread(state_s[1, 1, 2 * i].astype(F32) * end_s[1, 0:1, at])
        f2 = spread(state_s[1, 0, 2 * i + 1].astype(F32))
        dvb_s[:, at] = (dv_s[:, at] + nt(kf_s[:, at], e2) + nt(kb_s[:, at], f2)).astype(BF16)
        return 0

    def w_swap():
        arrived(wv_s.at[:, pl.ds(0, (nq - 1) * nq)], w2_rs)
        remote(wv_s, wv_s, w3_ss, w3_rs, there(chip, 1)).start()

    def send_dv(h, role, i):
        if role == 0:
            target = there(yy * nq + turned(xx, i, nq), 0)
        else:
            target = there(turned(yy, i, nq) * nq + xx, 1)
        src = dvb_s.at[:, pl.ds(role * HALF + h * 128, 128)]
        dst = dvg_s.at[h, x_slot[role]]

        def away():
            remote(src, dst, dv_ss, dv_rs.at[h], target).start()

        def at_home():
            pltpu.make_async_copy(src, dst, dv_rs.at[h]).start()

        if i == 0:
            pl.when(c != role)(away)
            pl.when(c == role)(at_home)
        else:
            away()

    def back(h):
        for way in range(2):

            @pl.when((c == 0) & (before(way) > 0))
            def _():
                arrived(state_s.at[1, way, pl.ds(0, quarter)], fw_rs.at[h, way])

    for h in range(PARTS):
        chain(1 - first, 2 * h * quarter, 2 * (h + 1) * quarter)
        back(h)
        lax.fori_loop(2 * h, 2 * h + 2, value_part, 0, unroll=2)
        for i in (2, 1, 3, 0) if nq == 4 else (1, 0):
            for role in range(2):
                send_dv(h, role, i)

    def finish(p, _):
        at = lanes(p * 128, 128)
        value = v_ref[:, at]
        cot = cot_ref[:, at]
        qf, kf, qb, kb = qf_s[:, at], kf_s[:, at], qb_s[:, at], kb_s[:, at]
        end = end_s[1, 0:1, at]
        place = place_of(p)
        h_state = state_s[1, 0, place].astype(F32)
        f_state = state_s[1, 0, place + 1].astype(F32)
        e_state = (state_s[1, 1, place].astype(F32) * end).astype(BF16).astype(F32)
        r_state = (state_s[1, 1, place + 1].astype(F32) * end).astype(BF16).astype(F32)
        carry = jnp.sum(
            e_state * (h_state + raw_s[2 * p]) + r_state * (f_state + raw_s[2 * p + 1]),
            axis=0,
            keepdims=True,
        )
        h2, f2, e2, r2 = spread(h_state), spread(f_state), spread(e_state), spread(r_state)
        dqf = dqf_s[:, at] + nn(cot, h2)
        dqb = dqb_s[:, at] + nn(cot, r2)
        dkf = dkf_s[:, at] + nn(value, e2)
        dkb = dkb_s[:, at] + nn(value, f2)
        running = run_s[:, at]
        exclusive = running - g_ref[:, at].astype(F32)
        dq = (jnp.exp(running) * dqf + jnp.exp(-exclusive) * dqb) * HEAD_DIM ** (-0.5)
        dk = jnp.exp(-running) * dkf + jnp.exp(exclusive) * dkb
        dq_ref[:, at] = dq.astype(BF16)
        dk_ref[:, at] = dk.astype(BF16)
        fwd = qf.astype(F32) * dqf - kf.astype(F32) * dkf
        bwd = kb.astype(F32) * dkb - qb.astype(F32) * dqb
        both_ways = fwd + bwd
        high = both_ways.astype(BF16)
        low = (both_ways - high.astype(F32)).astype(BF16)
        dg = nn(onward, high) + nn(onward, low) - bwd + carry
        dg_ref[:, at] = dg.astype(BF16)
        return 0

    pl.when((c == 1) & (edge >= 2))(turn_inputs)
    pl.when(c == 0)(w_swap)
    lax.fori_loop(0, PAIRS, finish, 0, unroll=UNROLL)

    outputs = [
        pltpu.make_async_copy(a, b, out_sem.at[n])
        for n, (a, b) in enumerate(
            ((dq_ref, dq_out), (dk_ref, dk_out), (dg_ref, dg_out), (gi_ref, gi_out))
        )
    ]
    for copy in outputs[:3]:
        copy.start()

    tokens = 2 * nq * BLOCK

    def s2_copies(h):
        return [
            remote(
                pb_s.at[h, turned(pb, i, nq)], s2_s.at[h, i - 1],
                s2_ss.at[h], s2_rs.at[h],
                there(chip_at(pa, turned(pb, i, nq)), c),
            )
            for i in range(1, nq)
        ]

    wide = PARTS
    stack = nz // wide
    height = 128 // stack

    per = stack // 2

    def summing(r, part):
        if r < per:
            return nz // 2 + part * per + r
        return (PARTS - 1 - part) * per + r - per

    def z_copy(to):
        return remote(zb_s.at[to], zr_s.at[z], zr_ss, zr_rs, there(chip, c, to))

    def reduce_part(h):
        total = part_s[h, pb]
        arrived(s2_s.at[h], s2_rs.at[h])
        for i in range(nq - 1):
            total = total + s2_s[h, i].astype(F32)
        for r in range(stack):
            zb_s[summing(r, h)] = total[r * height : (r + 1) * height].astype(BF16)
        for r in range(stack):
            to = summing(r, h)
            pl.when(to != z)(lambda: z_copy(to).start())

    for h in range(PARTS):
        arrived(dvg_s.at[h], dv_rs.at[h])
        part = nn(xgt_s[...], dvg_s[h].reshape(tokens, 128))
        part_s[h] = part.reshape(nq, 128, 128)
        pb_s[h] = part.astype(BF16).reshape(nq, 128, 128)
        for copy in s2_copies(h):
            copy.start()
        if h >= 2:
            reduce_part(h - 2)

    reduce_part(PARTS - 2)
    reduce_part(PARTS - 1)

    zr_s[z] = zb_s[z]

    arrived(zr_s.at[pl.ds(0, nz - 1)], zr_rs)
    rb_s[...] = jnp.sum(zr_s[...].astype(F32), axis=0).astype(BF16)

    upper_z = lax.div(2 * z, nz)
    owner = 1 - upper_z
    depth = lax.div(lax.rem(z, nz // 2), per)
    part_here = depth * upper_z + (PARTS - 1 - depth) * (1 - upper_z)
    slot = c * (nz // 2) + part_here * per + lax.rem(z, per)

    def out_copy(i):
        return remote(
            rb_s, gr_s.at[slot], za_ss, za_rs, there(chip, owner, turned(z, i, nz))
        )

    home = pltpu.make_async_copy(rb_s, gr_s.at[slot], za_rs)
    for near in range(nz // 2):
        out_copy(nz // 2 - near).start()
        if near > 0:
            out_copy(nz // 2 + near).start()
    pl.when(owner == c)(lambda: home.start())
    pl.when(owner != c)(lambda: out_copy(0).start())

    pl.when(c == 1)(lambda: arrived(wv_s, w3_rs))
    group = nq * 128
    for i in range(nq):
        low_half = wv_s[0, i * nq : (i + 1) * nq].reshape(group, HALF)
        high_half = wv_s[1, i * nq : (i + 1) * nq].reshape(group, HALF)
        gi_ref[:, i * group : (i + 1) * group] = (
            nt(dvb_s[:, :HALF], low_half) + nt(dvb_s[:, HALF:], high_half)
        ).astype(BF16)

    outputs[3].start()

    arrived(gr_s, za_rs)

    for copy in outputs:
        copy.wait()
    left(zr_s.at[pl.ds(0, nz - 1)], zr_ss)
    for h in range(PARTS):
        left(s2_s.at[h], s2_ss.at[h])
    pl.when(owner == c)(lambda: left(zr_s.at[pl.ds(0, nz - 1)], za_ss))
    pl.when(owner != c)(lambda: left(zr_s, za_ss))

    @pl.when(c == 0)
    def _():
        left(loc_s.at[1, lead], loc_ss.at[0])
        left(end_s.at[1], loc_ss.at[1])

    left(end_s.at[1], fend_ss)
    left(fol_s.at[0], fol_ss)

    @pl.when((c == 1) & (before(lead) < nz - 1))
    def _():
        for s in range(2):
            left(out_s.at[s], chain_ss.at[s])

    @pl.when((c == 1) & (before(lead) > 1))
    def _():
        for s in range(2):
            left(in_s.at[s], hand_ss.at[s])

    for way in range(2):

        @pl.when((c == 1) & (before(way) > 0))
        def _():
            left(state_s.at[0, way], fw_ss.at[way])

    @pl.when(c == 0)
    def _():
        left(wv_s.at[:, pl.ds(0, nq - 1)], w1_ss)
        left(wv_s.at[:, pl.ds(0, (nq - 1) * nq)], w2_ss)
        left(wv_s, w3_ss)

    @pl.when(c == 1)
    def _():
        left(w_shard, w0_ss)

    left(xg_s.at[pl.ds(0, 2 * nq - 1)], x_ss)
    left(dvg_s.at[:, pl.ds(0, 2 * nq - 1)], dv_ss)


def store(dq, dk, dg, gi, gr, dq_out, dk_out, dg_out, gi_out, gw_out, gw_s, sems):
    copies = [
        pltpu.make_async_copy(a, b, sems.at[n])
        for n, (a, b) in enumerate(((gi, gi_out), (dq, dq_out), (dk, dk_out), (dg, dg_out)))
    ]
    for copy in copies:
        copy.start()
    count, height, chunk = gr.shape
    for s in range(count):
        role, t = s // (count // 2), s % (count // 2)
        per = count // 2 // PARTS
        rows, columns = t % per * height, role * HALF + t // per * chunk
        gw_s[rows : rows + height, columns : columns + chunk] = gr[s].astype(F32)
    last = pltpu.make_async_copy(gw_s, gw_out, sems.at[4])
    last.start()
    for copy in (*copies, last):
        copy.wait()


def per_device(nz, nq, inputs, queries, keys, values, log_decay, cotangent, value_weight):
    model = inputs.shape[2]
    slots = 2 * nq
    wide = PARTS
    chunk = (128 * wide // nz, HALF // wide)
    dma = pltpu.SemaphoreType.DMA
    vm = pltpu.VMEM
    shapes = [((BLOCK, WIDTH), BF16)] * 3 + [((BLOCK, model), BF16)]
    sums = ((nz, *chunk), BF16)
    weight = ((64, WIDTH), F32)
    in_vmem = pl.BlockSpec(memory_space=pltpu.VMEM)
    anywhere = pl.BlockSpec(memory_space=pl.ANY)
    outs = pl.pallas_call(
        functools.partial(kernel, nz, nq),
        out_shape=tuple(vm(*shape) for shape in (*shapes, sums)),
        in_specs=[anywhere] * 7,
        out_specs=[anywhere] * 5,
        scratch_shapes=[
            *[vm((BLOCK, WIDTH), BF16)] * 8,
            vm((BLOCK, model), BF16),
            vm((BLOCK, WIDTH), F32),
            vm((2, 8, WIDTH), F32),
            *[vm((BLOCK, WIDTH), BF16)] * 4,
            vm((2, 2, CHUNKS, 64, 128), BF16),
            vm((CHUNKS, 64, 128), F32),
            vm((2, CHUNKS, 64, 128), BF16),
            vm((2, 8, WIDTH), F32),
            vm((2, CHUNKS, 64, 128), BF16),
            vm((2, CHUNKS, 64, 128), BF16),
            vm((2, 2, CHUNKS, 64, 128), BF16),
            *[vm((BLOCK, WIDTH), F32)] * 5,
            vm((BLOCK, WIDTH), BF16),
            vm((2, nq * nq, 128, HALF), BF16),
            vm((slots, BLOCK, nq * 128), BF16),
            vm((nq * 128, slots * BLOCK), BF16),
            vm((PARTS, slots, BLOCK, 128), BF16),
            vm((PARTS, nq, 128, 128), F32),
            vm((PARTS, nq, 128, 128), BF16),
            vm((PARTS, nq - 1, 128, 128), BF16),
            vm(*sums),
            vm(*sums),
            vm(chunk, BF16),
            dma((2,)), dma((4,)),
            dma((2,)), dma((2, CHUNKS)),
            dma((2,)), dma((2, PARTS)),
            dma((2,)), dma((PARTS, 2)),
            dma((2,)), dma((2, 2)),
            dma, dma((2, PARTS)),
            dma, dma((2, 2)),
            *[dma] * 4,
            dma((2,)),
            *[dma] * 7,
            dma((PARTS,)),
            dma((PARTS,)), dma((PARTS,)),
            *[dma] * 4,
        ],
        compiler_params=pltpu.CompilerParams(
            collective_id=0, has_side_effects=True, vmem_limit_bytes=65_300_000
        ),
    )(
        queries[0], keys[0], values[0], log_decay[0], cotangent[0], inputs[0], value_weight
    )
    dq, dk, dg, gi, gw = pl.pallas_call(
        store,
        out_shape=tuple(jax.ShapeDtypeStruct(*shape) for shape in (*shapes, weight)),
        in_specs=[anywhere] * 4 + [in_vmem],
        out_specs=[anywhere] * 5,
        scratch_shapes=[vm(*weight), dma((5,))],
        compiler_params=pltpu.CompilerParams(vmem_limit_bytes=1024 * 1024),
    )(*outs)
    return dq[None], dk[None], dg[None], gi[None], gw


def solution(mesh):
    nz = mesh.shape["sp"]
    nq = 4 if mesh.shape["dp"] == 32 else 2
    tokens = P("dp", "sp", None)
    return jax.shard_map(
        functools.partial(per_device, nz, nq),
        mesh=mesh,
        in_specs=(tokens,) * 6 + (P("dp", None),),
        out_specs=(tokens,) * 4 + (P("dp", None),),
        check_vma=False,
    )
```
